512 devices in a mesh: sp: 32 (over z, x), tp: 16 (over y, core).
Axes of the slice: x: 4, y: 8, z: 8, core: 2. Of those that a mesh axis runs over, the one named last changes fastest.
Arguments:
- queries: bfloat16 [8192, 2048], P('sp', 'tp'), may hold values from -6 to 6
- keys: bfloat16 [8192, 1024], P('sp', 'tp'), may hold values from -6 to 6
- values: bfloat16 [8192, 1024], P('sp', 'tp'), may hold values from -6 to 6
- docs: int32 [8192], P('sp'), may hold values from 0 to 2, never falling along the last dimension, each value on 1 to 5120 neighbouring positions
- query_gain: float32 [64], replicated, may hold values from 0.5 to 8
- key_gain: float32 [64], replicated, may hold values from 0.5 to 8
- out_weight: bfloat16 [2048, 2048], P('tp'), may hold values from -0.125 to 0.125
- residual: bfloat16 [8192, 2048], P('sp', 'tp'), may hold values from -12 to 12
- norm_gain: float32 [2048], P('tp'), may hold values from 0.1 to 1.9
- routes: int32 [8192, 2], P('sp'), may hold values from 0 to 31, all different within a row; in each aligned block of 256 rows (0 to 255, 256 to 511, ...) at most 20 rows name the same one
- route_weight: float32 [8192, 2], P('sp'), may hold values from 0.1 to 1
- gate_weight: bfloat16 [32, 2048, 4096], P('sp', None, 'tp'), may hold values from -0.3125 to 0.3125
- up_weight: bfloat16 [32, 2048, 4096], P('sp', None, 'tp'), may hold values from -0.3125 to 0.3125
- down_weight: bfloat16 [32, 4096, 2048], P('sp', 'tp'), may hold values from -0.09375 to 0.09375
Outputs:
- mixed: bfloat16 [8192, 2048], P('sp', 'tp')
The draws below stay inside these ranges and needn't reach their ends.
Inputs may be any that keep to these rules, and one draw needn't show every extreme that they name: `routes`: in each aligned block of 256 rows no expert is named by more than 20 rows, and 20 is reached in some block; a row names 2 different experts. `docs`: document numbers never fall along the sequence; a document holds at most 5120 positions.
All inputs are finite; a program needn't handle non-finite values.
Results may differ from the reference program's by a relative error of at most 0.028.
The reference program's roundings to bfloat16 on the way count: a program that leaves them out, or rounds other values in their place, can miss the bound.
Values may be sent and summed in bfloat16 or wider, within the bound.
No kernel may reach another device: no remote copies, remote signals or barrier semaphores. Data moves between devices by JAX's collectives and lax.ppermute only.
A program may use at most 64 MiB of HBM per device.

```python
import math
import jax
import jax.numpy as jnp
import numpy as np
from jax import lax

D = 2048
QH = 32
KVH = 16
HD = 64
EFF = 4096
TOPK = 2
GRID_W = 64
DOCS = 3
TOK_DEV = 256
SEQ = 8192
EXPERTS = 32
CAP = 20
DOC_MOST = 5120
N_SP = 32
N_TP = 16


def base_queries(key):
    raw = jax.random.normal(jax.random.fold_in(key, 11), (SEQ, QH * HD), jnp.float32)
    return jnp.clip(raw, -6.0, 6.0)


def draw_queries(key, part):
    return base_queries(key).astype(jnp.bfloat16)


def draw_keys(key, part):
    entries = jnp.clip(jax.random.normal(jax.random.fold_in(key, 12), (SEQ, KVH * HD), jnp.float32), -6.0, 6.0)
    return entries.astype(jnp.bfloat16)


def draw_query_gain(key, part):
    return jax.random.uniform(jax.random.fold_in(key, 21), (HD,), jnp.float32, 0.5, 1.5)


def draw_key_gain(key, part):
    return jax.random.uniform(jax.random.fold_in(key, 22), (HD,), jnp.float32, 0.5, 1.5)


def draw_residual(key, part):
    column = jnp.arange(D, dtype=jnp.float32) / D
    entries = jnp.clip(jax.random.normal(jax.random.fold_in(key, 31), (SEQ, D), jnp.float32), -4.0, 4.0)
    column_scale = jnp.exp(column * math.log(3.0))
    row_scale = jnp.exp(jax.random.uniform(jax.random.fold_in(key, 32), (SEQ, 1), jnp.float32, math.log(0.1), 0.0))
    return (entries * row_scale * column_scale[None, :]).astype(jnp.bfloat16)


def shard_levels(rng, dims, shards, least, largest):
    factor_of, own = 1.0, jax.random.fold_in(rng, 6)
    for dim, shards_of in shards:
        draws = jnp.exp(jax.random.uniform(jax.random.fold_in(own, dim), (shards_of,), jnp.float32, least / len(shards), largest / len(shards)))
        factor_of = factor_of * jnp.repeat(draws, dims[dim] // shards_of).reshape([-1 if axis == dim else 1 for axis in range(len(dims))])
    return factor_of


def split_up(count, total, reach, skew):
    loads = [(1 << 20) // math.isqrt(grade ** skew) + 1 for grade in range(2, count + 1)]
    surplus, given = total - reach - (count - 1), [1] * (count - 1)
    while surplus > 0:
        free = [i for i in range(count - 1) if given[i] < reach]
        mass, remaining = sum([loads[i] for i in free]), surplus
        for i in free:
            more = min(reach - given[i], max(1, remaining * loads[i] // mass), surplus)
            given[i] = given[i] + more
            surplus = surplus - more
    return np.array([reach] + given)


def uneven(own_key, count, total, bound, skew):
    if count == 2:
        one = jax.random.randint(own_key, (), max(1, total - bound), min(bound, total - 1) + 1)
        return jnp.stack([one, total - one])
    sizes = jnp.asarray(split_up(count, total, bound, skew), jnp.int32)
    twos = (count - 1) // 2
    giver, receiver = sizes[1:1 + 2 * twos:2], sizes[2:2 + 2 * twos:2]
    margin = jnp.minimum(giver - 1, bound - receiver)
    moved = jax.random.randint(jax.random.fold_in(own_key, 1), (twos,), 0, 1 << 20) % (margin + 1)
    sizes = sizes.at[1:1 + 2 * twos:2].set(giver - moved).at[2:2 + 2 * twos:2].set(receiver + moved)
    return sizes[jax.random.permutation(jax.random.fold_in(own_key, 2), count)]


def assign_block(stream_key, own, number, rows, count, top, bound, slope):
    ranking = jax.random.permutation(stream_key, count)
    crowded, usual = load_shares(count, rows * top, bound, slope, True), load_shares(count, rows * top, bound, slope, False)
    places = jnp.arange(count)

    def named(lengths, turn):
        used = int((lengths > 0).sum())
        fixed = max(1, used // 4)
        shifted = fixed + (places - fixed + turn * (used - fixed)) % max(1, count - fixed)
        return jnp.zeros((count,), jnp.int32).at[ranking[jnp.where(places < fixed, places, shifted)]].set(jnp.asarray(lengths, jnp.int32))

    lengths = jnp.where(number % 4 == 0, named(crowded, number // 4), named(usual, number - number // 4 - 1))
    mixed = jax.random.permutation(jax.random.fold_in(own, 3), count)
    donor, receiver = mixed[0:count // 2 * 2:2], mixed[1:count // 2 * 2:2]
    room = jnp.minimum(lengths[donor] - 1, bound - lengths[receiver]) // 2
    room = jnp.where((donor == ranking[0]) | (receiver == ranking[0]) | (lengths[receiver] == 0), 0, jnp.maximum(room, 0))
    shifted = jax.random.randint(jax.random.fold_in(own, 4), (count // 2,), 0, 1 << 20) % (room + 1)
    lengths = lengths.at[donor].add(-shifted).at[receiver].add(shifted)
    items = jnp.searchsorted(jnp.cumsum(lengths), jnp.arange(rows * top), side="right").astype(jnp.int32)
    grid = items.reshape(top, rows).T
    grid = grid[jax.random.permutation(jax.random.fold_in(own, 1), rows)]
    turn = jax.random.randint(jax.random.fold_in(own, 2), (rows, 1), 0, top)
    return jnp.take_along_axis(grid, (jnp.arange(top)[None, :] + turn) % top, axis=1)


def load_shares(count, total, most, slope, full):
    weights = [(1 << 20) // math.isqrt(grade ** slope) + 1 for grade in range(1, count + 1)]
    largest = most if full else min(most, max(-(-total // count), total * weights[0] // sum(weights)))
    least = 1 if total - largest >= count - 1 else 0
    counts, surplus = [largest] + [least] * (count - 1), total - largest - least * (count - 1)
    while surplus > 0:
        movable = [i for i in range(1, count) if counts[i] < largest] or [i for i in range(1, count) if counts[i] < most]
        pool, budget = sum([weights[i] for i in movable]), surplus
        for i in movable:
            addition = min(most - counts[i], max(1, budget * weights[i] // pool), surplus)
            counts[i] = counts[i] + addition
            surplus = surplus - addition
    return np.array(counts)


def normal_values(stream_key, dims, spread, most, cuts=(), kind=jnp.bfloat16):
    values = jax.random.normal(stream_key, dims, jnp.float32) * spread
    if len(cuts) > 0:
        values = shard_levels(stream_key, dims, cuts, -0.22, 0.18) * values
    return jnp.clip(values, min=-most, max=most).astype(kind)


def setup_inputs(seed: int = 0) -> dict:
    arg_keys = jax.random.split(jax.random.key(seed), 15)
    queries = draw_queries(jax.random.fold_in(arg_keys[14], 71), 0)
    keys = draw_keys(jax.random.fold_in(arg_keys[14], 71), 0)
    values = normal_values(arg_keys[2], (SEQ, KVH * HD), 1.0, 6.0, ((0, 32), (1, 16)))
    docs = jnp.searchsorted(jnp.cumsum(uneven(arg_keys[3], DOCS, SEQ, DOC_MOST, 0)), jnp.arange(SEQ), side="right").astype(jnp.int32)
    query_gain = draw_query_gain(jax.random.fold_in(arg_keys[14], 71), 0)
    key_gain = draw_key_gain(jax.random.fold_in(arg_keys[14], 71), 0)
    out_weight = normal_values(arg_keys[6], (QH * HD, D), (QH * HD) ** -0.5, 0.125, ((0, 16),))
    residual = draw_residual(jax.random.fold_in(arg_keys[14], 71), 0)
    norm_gain = jnp.clip(1.0 + 0.18 * jax.random.normal(arg_keys[8], (D,), jnp.float32), 0.1, 1.9)
    routes_keys = jax.random.split(jax.random.fold_in(arg_keys[9], 1), SEQ // TOK_DEV)
    routes_turns = jax.random.permutation(jax.random.fold_in(arg_keys[9], 3), SEQ // TOK_DEV)
    routes = jax.vmap(lambda own, number: assign_block(jax.random.fold_in(arg_keys[9], 2), own, number, TOK_DEV, EXPERTS, TOPK, CAP, 2))(routes_keys, routes_turns).reshape((SEQ, TOPK))
    route_weight = jnp.clip(jnp.exp(math.log(1.0) - 2.3025851 * jax.random.uniform(arg_keys[10], (SEQ, TOPK), jnp.float32) ** shard_levels(arg_keys[10], (SEQ, TOPK), ((0, 32),), -0.2, 0.2)), 0.1, 1.0)
    gate_weight = normal_values(arg_keys[11], (EXPERTS, D, EFF), (D // 6) ** -0.5, 0.3125, ((0, 32), (2, 16)))
    up_weight = normal_values(arg_keys[12], (EXPERTS, D, EFF), (D // 6) ** -0.5, 0.3125, ((0, 32), (2, 16)))
    down_weight = normal_values(arg_keys[13], (EXPERTS, EFF, D), EFF ** -0.5, 0.09375, ((0, 32), (1, 16)))
    return {"queries": queries, "keys": keys, "values": values, "docs": docs, "query_gain": query_gain, "key_gain": key_gain, "out_weight": out_weight, "residual": residual, "norm_gain": norm_gain, "routes": routes, "route_weight": route_weight, "gate_weight": gate_weight, "up_weight": up_weight, "down_weight": down_weight}


EPSILON = 1e-06
NEG_BIG = -1e+30
ROTARY_BASE = 10000.0
CLAMP_LIMIT = 7.0
SIGMOID_SCALE = 1.702

def rope_tables(positions, head_dim):
    quarter = head_dim // 4
    freqs = ROTARY_BASE ** (-jnp.arange(quarter, dtype=jnp.float32) / quarter)
    row_pos = (positions // GRID_W).astype(jnp.float32)
    col_pos = (positions % GRID_W).astype(jnp.float32)
    angle = jnp.concatenate([row_pos[:, None] * freqs, col_pos[:, None] * freqs], axis=1)
    return (jnp.cos(angle), jnp.sin(angle))

def norm_rotate(heads, gain, cosine_table, sine_table):
    entries = heads.astype(jnp.float32)
    entries = entries * lax.rsqrt(lax.optimization_barrier(jnp.mean(entries * entries, axis=-1, keepdims=True)) + EPSILON) * gain
    pairs = entries.reshape(entries.shape[:-1] + (entries.shape[-1] // 2, 2))
    first = pairs[..., 0]
    second = pairs[..., 1]
    cos_rows = cosine_table[:, None, :]
    sin_rows = sine_table[:, None, :]
    turned = jnp.stack([first * cos_rows - second * sin_rows, first * sin_rows + second * cos_rows], axis=-1)
    return turned.reshape(heads.shape).astype(jnp.bfloat16)

def clamped_unit(gate_pre, up_pre):
    bounded = jnp.minimum(gate_pre, CLAMP_LIMIT)
    linear = jnp.clip(up_pre, -CLAMP_LIMIT, CLAMP_LIMIT)
    return (bounded * jax.nn.sigmoid(SIGMOID_SCALE * bounded) * (linear + 1.0)).astype(jnp.bfloat16)

def round_trip(term):
    narrow = lax.optimization_barrier(term.astype(jnp.bfloat16))
    return narrow.astype(jnp.float32)

def reference(queries, keys, values, docs, query_gain, key_gain, out_weight, residual, norm_gain, routes, route_weight, gate_weight, up_weight, down_weight):
    positions = jnp.arange(SEQ, dtype=jnp.int32)
    cosine_table, sine_table = rope_tables(positions, HD)
    query_rot = norm_rotate(queries.reshape(SEQ, QH, HD), query_gain, cosine_table, sine_table)
    key_rot = norm_rotate(keys.reshape(SEQ, KVH, HD), key_gain, cosine_table, sine_table)
    query_grouped = jnp.transpose(query_rot.reshape(SEQ, KVH, 2, HD), (1, 0, 2, 3))
    key_grouped = jnp.transpose(key_rot, (1, 0, 2))
    value_grouped = jnp.transpose(values.reshape(SEQ, KVH, HD), (1, 0, 2))
    block_rows = math.gcd(SEQ, 1024)
    score_scale = HD ** (-0.5)

    def one_head(inputs):
        head_queries, head_keys, head_values = inputs
        keys_wide = head_keys.astype(jnp.float32)
        values_wide = head_values.astype(jnp.float32)

        def one_block(index):
            start = (index * block_rows).astype(jnp.int32)
            block_queries = lax.dynamic_slice_in_dim(head_queries, start, block_rows, 0).astype(jnp.float32)
            block_docs = lax.dynamic_slice_in_dim(docs, start, block_rows, 0)
            scores = jnp.einsum('qgd,kd->qgk', block_queries, keys_wide) * score_scale
            allowed = block_docs[:, None, None] == docs[None, None, :]
            scores = jnp.where(allowed, scores, NEG_BIG)
            row_peak = lax.optimization_barrier(jnp.max(scores, axis=-1, keepdims=True))
            weights = jnp.where(allowed, jnp.exp(scores - row_peak), 0.0)
            denominator = lax.optimization_barrier(jnp.sum(weights, axis=-1))
            numerator = jnp.einsum('qgk,kd->qgd', round_trip(weights), values_wide)
            return (numerator / denominator[..., None]).astype(jnp.bfloat16)
        return lax.map(one_block, jnp.arange(SEQ // block_rows, dtype=jnp.int32))
    heads_out = lax.map(one_head, (query_grouped, key_grouped, value_grouped))
    attended = jnp.transpose(heads_out.reshape(KVH, SEQ, 2, HD), (1, 0, 2, 3)).reshape(SEQ, QH * HD)
    group_width = QH * HD // N_TP
    grouped_attn = jnp.transpose(attended.reshape(SEQ, N_TP, group_width), (1, 0, 2))
    grouped_weight = out_weight.reshape(N_TP, group_width, D)

    def add_group(running, inputs):
        part_attn, part_weight = inputs
        return (running + round_trip(jnp.dot(part_attn, part_weight, preferred_element_type=jnp.float32)), None)
    projected, _ = lax.scan(add_group, jnp.zeros((SEQ, D), jnp.float32), (grouped_attn, grouped_weight))
    mixed_first = residual.astype(jnp.float32) + projected
    normed = (mixed_first * lax.rsqrt(lax.optimization_barrier(jnp.mean(mixed_first * mixed_first, axis=1, keepdims=True)) + EPSILON) * norm_gain).astype(jnp.bfloat16)
    pair_count = TOK_DEV * TOPK
    group_routes = routes.reshape(N_SP, pair_count)
    expert_ids = jnp.arange(EXPERTS, dtype=jnp.int32)
    onehot = (group_routes[:, :, None] == expert_ids[None, None, :]).astype(jnp.int32)
    earlier = jnp.cumsum(onehot, axis=1) - onehot
    slot_index = lax.optimization_barrier(jnp.sum(earlier * onehot, axis=2))
    slot_ids = jnp.arange(CAP, dtype=jnp.int32)
    matches = (group_routes[:, :, None, None] == expert_ids[None, None, :, None]) & (slot_index[:, :, None, None] == slot_ids[None, None, None, :])
    entry_ids = jnp.arange(pair_count, dtype=jnp.int32)
    source_entry = lax.optimization_barrier(jnp.sum(jnp.where(matches, entry_ids[None, :, None, None], 0), axis=1))
    occupied = jnp.any(matches, axis=1)
    token_index = (jnp.arange(N_SP, dtype=jnp.int32)[:, None, None] * TOK_DEV + source_entry // TOPK).astype(jnp.int32)
    expert_in = jnp.where(occupied[..., None], normed[token_index], jnp.zeros((), jnp.bfloat16))
    expert_in = jnp.transpose(expert_in, (1, 0, 2, 3)).reshape(EXPERTS, N_SP * CAP, D)
    hidden_group = EFF // N_TP
    slot_rows = N_SP * CAP

    def one_expert(inputs):
        rows, gate_part, up_part, down_part = inputs
        gate_pre = jnp.dot(rows, gate_part, preferred_element_type=jnp.float32)
        up_pre = jnp.dot(rows, up_part, preferred_element_type=jnp.float32)
        hidden = clamped_unit(gate_pre, up_pre)
        hidden_groups = jnp.transpose(hidden.reshape(slot_rows, N_TP, hidden_group), (1, 0, 2))
        down_groups = down_part.reshape(N_TP, hidden_group, D)

        def add_part(running, pieces):
            part_hidden, part_down = pieces
            return (running + round_trip(jnp.dot(part_hidden, part_down, preferred_element_type=jnp.float32)), None)
        summed, _ = lax.scan(add_part, jnp.zeros((slot_rows, D), jnp.float32), (hidden_groups, down_groups))
        return summed.astype(jnp.bfloat16)
    expert_out = lax.map(one_expert, (expert_in, gate_weight, up_weight, down_weight))
    lookup = ((group_routes * N_SP + jnp.arange(N_SP, dtype=jnp.int32)[:, None]) * CAP + slot_index).astype(jnp.int32)
    picked = expert_out.reshape(EXPERTS * slot_rows, D)[lookup.reshape(-1)].reshape(SEQ, TOPK, D).astype(jnp.float32)
    routed = lax.optimization_barrier(jnp.sum(route_weight[:, :, None] * picked, axis=1))
    return (mixed_first + routed).astype(jnp.bfloat16)
```

```python
import functools

import jax
import jax.numpy as jnp
import numpy as np
from jax import lax
from jax.experimental import pallas as pl
from jax.experimental.pallas import tpu as pltpu
from jax.sharding import Mesh, PartitionSpec as P

GRID_W = 64
EPSILON = 1e-06
ROTARY_BASE = 10000.0
CLAMP_LIMIT = 7.0
SIGMOID_SCALE = 1.702
N_Z, N_X, N_Y, N_C = 8, 4, 8, 2
N_SP, N_TP = N_Z * N_X, N_Y * N_C
TOK = 256
HALF = TOK // 2
HD = 64
LANES = 128
D = 2048
EXPERTS = 32
CAP = 20
CAP_PAD = 24
ROWS = N_SP * CAP // 2
HID = 256
NOTE = 16
MASK_BIG = 16384.0

F32 = jnp.float32
BF16 = jnp.bfloat16


def tables():
    quarter = HD // 4
    freqs = (ROTARY_BASE ** (-np.arange(quarter, dtype=np.float32) / quarter)).astype(np.float32)
    lane = np.arange(LANES)
    pair = (lane % HD) // 2
    is_row = pair < quarter
    freq = freqs[np.where(is_row, pair, pair - quarter)]
    sign = np.where(lane % 2 == 0, -1.0, 1.0)
    cols = (np.arange(GRID_W, dtype=np.float32)[:, None] * freq).astype(np.float32)
    rows = (np.arange(N_SP * TOK // GRID_W, dtype=np.float32)[:, None] * freq).astype(np.float32)
    cols, rows = cols.astype(np.float64), rows.astype(np.float64)
    keep = lambda a, m: np.where(m, a, 0.0).astype(np.float32)
    per = TOK // GRID_W
    row_c = keep(np.cos(rows), is_row).reshape(N_SP, per, LANES)
    row_s = keep(np.sin(rows) * sign, is_row).reshape(N_SP, per, LANES)
    row_tab = np.concatenate([row_c, row_s], axis=1)
    col_tab = np.stack([keep(np.cos(cols), ~is_row), keep(np.sin(cols) * sign, ~is_row)])
    return row_tab, col_tab


def compaction():
    out = np.zeros((ROWS, 16 * CAP_PAD), np.float32)
    r = np.arange(ROWS)
    out[r, (r // CAP) * CAP_PAD + r % CAP] = 1.0
    return out


def dot(a, b, ca=1, cb=0):
    return lax.dot_general(a, b, (((ca,), (cb,)), ((), ())), preferred_element_type=F32)


def iota(shape, dim):
    return lax.broadcasted_iota(jnp.int32, shape, dim)


def prep_body(blk, q_ref, k_ref, v_ref, docs_ref, qg_ref, kg_ref, row_ref, col_ref, qs_ref, kvs_ref):
    lane = iota((TOK, LANES), 1)
    low = lane < HD
    even = (lane & 1) == 0
    rows = row_ref[blk[0]]
    per = TOK // GRID_W
    cos_t = jnp.concatenate([col_ref[0] + rows[j : j + 1] for j in range(per)], axis=0)
    sin_t = jnp.concatenate([col_ref[1] + rows[per + j : per + j + 1] for j in range(per)], axis=0)

    def turn(n):
        swapped = jnp.where(even, pltpu.roll(n, LANES - 1, 1), pltpu.roll(n, 1, 1))
        return n * cos_t + swapped * sin_t

    x = q_ref[...].astype(F32)
    sq = x * x
    s0 = jnp.sum(jnp.where(low, sq, 0.0), axis=1, keepdims=True)
    s1 = jnp.sum(jnp.where(low, 0.0, sq), axis=1, keepdims=True)
    r0 = lax.rsqrt(s0 * (1.0 / HD) + EPSILON)
    r1 = lax.rsqrt(s1 * (1.0 / HD) + EPSILON)
    gain = jnp.concatenate([qg_ref[...], qg_ref[...]], axis=1)
    q_out = turn(x * jnp.where(low, r0, r1) * gain).astype(BF16)

    kv = jnp.concatenate([k_ref[...], v_ref[...]], axis=0).astype(F32).T
    sk = jnp.sum(jnp.where(low, kv * kv, 0.0), axis=1, keepdims=True)
    rk = lax.rsqrt(sk * (1.0 / HD) + EPSILON)
    gain_k = jnp.concatenate([kg_ref[...], kg_ref[...]], axis=1)
    kv_out = jnp.where(low, turn(kv * rk * gain_k), kv).astype(BF16)

    docs = docs_ref[...]
    n0 = jnp.sum((docs < 1).astype(F32))
    n1 = jnp.sum((docs < 2).astype(F32))
    row = iota((NOTE, LANES), 0)
    note = jnp.where(row == 0, n0, jnp.where(row == 1, n1, 0.0)).astype(BF16)
    for i in range(N_X):
        qs_ref[i, :TOK, :] = q_out
        qs_ref[i, TOK:, :] = note
    for i in range(N_Z):
        kvs_ref[i, :TOK, :] = kv_out
        kvs_ref[i, TOK:, :] = note


def split3(x):
    hi = x.astype(BF16).astype(F32)
    mid = (x - hi).astype(BF16).astype(F32)
    return hi, mid, x - hi - mid


def attend_body(q_ref, kv_ref, out_ref, kp_ref, vp_ref):
    lane = iota((TOK, LANES), 1)
    low = lane < HD
    idx = iota((TOK, LANES), 0).astype(F32)

    def doc_of(note):
        n0 = note[0:1, :].astype(F32)
        n1 = note[1:2, :].astype(F32)
        return jnp.where(idx < n0, HD, jnp.where(idx < n1, HD + 1, HD + 2))

    for j in range(N_Z):
        kv = kv_ref[j, :TOK, :]
        mark = (doc_of(kv_ref[j, TOK:, :]) == lane).astype(F32)
        kvf = kv.astype(F32)
        kp_ref[j * TOK : (j + 1) * TOK, :] = jnp.where(low, kvf, mark).astype(BF16)
        vp_ref[j * TOK : (j + 1) * TOK, :] = jnp.where(low, 1.0, kvf).astype(BF16)
    eye = (iota((HALF, LANES), 0) == iota((HALF, LANES), 1)).astype(BF16)
    lane_h = iota((HALF, LANES), 1)

    def block(b, carry):
        qf = q_ref[b, :TOK, :].astype(F32) * (HD**-0.5)
        doc = doc_of(q_ref[b, TOK:, :])
        other = jnp.where((doc == lane) | (lane > HD + 2), 0.0, -MASK_BIG)
        heads = []
        for h in range(2):
            qh = qf if h == 0 else pltpu.roll(qf, HD, 1)
            qp = jnp.where(low, qh, other).astype(BF16)
            s = dot(qp, kp_ref[...], 1, 1)
            peak = jnp.max(s, axis=1, keepdims=True)
            p = jnp.exp(s - peak).astype(BF16)
            acc = dot(p, vp_ref[...])
            total = acc[:, 0:1]
            o = acc / total
            heads.append((pltpu.roll(o, HD, 1) if h == 0 else o, peak + jnp.log(total)))
        o = jnp.where(low, heads[0][0], heads[1][0]).astype(BF16)
        parts = split3(heads[0][1]) + split3(heads[1][1])
        for half in range(2):
            rows = slice(half * HALF, (half + 1) * HALF)
            stat = jnp.zeros((HALF, LANES), F32)
            for i, part in enumerate(parts):
                stat = jnp.where(lane_h == i, part[rows], stat)
            stat_t = dot(stat.astype(BF16), eye, 0, 0)
            out_ref[b * 2 + half, :HALF, :] = o[rows]
            out_ref[b * 2 + half, HALF:, :] = stat_t[:NOTE].astype(BF16)
        return carry

    lax.fori_loop(0, N_X, block, 0)


def project_body(core, in_ref, w_own_ref, w_other_ref, out_ref):
    row = iota((NOTE, LANES), 0)
    lane = iota((NOTE, LANES), 1)
    pick = (((row < 3) & (lane < HD)) | ((row >= 3) & (row < 6) & (lane >= HD))).astype(BF16)

    def attended(c):
        lse = [dot(in_ref[x * 2 + c, HALF:, :], pick, 0, 0) for x in range(N_X)]
        top = functools.reduce(jnp.maximum, lse)
        total = jnp.zeros((HALF, LANES), F32)
        mixed = jnp.zeros((HALF, LANES), F32)
        for x in range(N_X):
            w = jnp.exp(lse[x] - top)
            total = total + w
            mixed = mixed + w * in_ref[x * 2 + c, :HALF, :].astype(F32)
        return (mixed / total).astype(BF16)

    own = attended(core[0])
    other = attended(1 - core[0])
    for g in range(N_TP):
        cols = slice(g * LANES, (g + 1) * LANES)
        part = dot(own, w_own_ref[:, cols]) + dot(other, w_other_ref[:, cols])
        out_ref[g] = part.astype(BF16)


def route_body(routes_ref, weight_ref, place_ref, mix_ref):
    expert = iota((EXPERTS, TOK), 0)
    r0, r1 = routes_ref[0:1, :], routes_ref[1:2, :]
    named = ((expert == r0) | (expert == r1)).astype(F32)
    before = (iota((TOK, TOK), 0) < iota((TOK, TOK), 1)).astype(BF16)
    slot = dot(named.astype(BF16), before)
    weight = jnp.where(expert == r0, weight_ref[0:1, :], jnp.where(expert == r1, weight_ref[1:2, :], 0.0))
    slot = jnp.where(named > 0.0, slot, -1.0)
    w3 = split3(weight)
    slots = iota((CAP_PAD, TOK), 0).astype(F32)
    for e in range(EXPERTS):
        rows = slice(e * CAP_PAD, (e + 1) * CAP_PAD)
        hit = slots == slot[e : e + 1, :]
        place_ref[rows, :] = hit.astype(F32)
        for i in range(3):
            mix_ref[i, rows, :] = jnp.where(hit, w3[i][e : e + 1, :], 0.0)


def dispatch_body(in_ref, residual_ref, place_ref, mixed_ref, out_ref):
    halves = []
    for c in range(2):
        total = in_ref[c].astype(F32)
        for y in range(1, N_Y):
            total = total + in_ref[y * 2 + c].astype(F32)
        halves.append(total)
    mixed = residual_ref[...].astype(F32) + jnp.concatenate(halves, axis=0)
    mixed_ref[...] = mixed
    out_ref[...] = dot(place_ref[...].astype(BF16), mixed.astype(BF16)).astype(BF16)


def spread_body(in_ref, drop_ref, out_ref):
    for c in range(2):
        rows = in_ref[c * 16 * CAP_PAD : (c + 1) * 16 * CAP_PAD, :]
        kept = dot(drop_ref[...], rows).astype(BF16)
        for y in range(N_Y):
            out_ref[y * 2 + c] = kept


def expert_body(in_ref, gain_ref, g0_ref, g1_ref, u0_ref, u1_ref, d0_ref, d1_ref, out_ref, x_ref):
    total = jnp.zeros((ROWS, LANES), F32)
    for g in range(N_TP):
        x = in_ref[g].astype(F32)
        total = total + x * x
    scale = lax.rsqrt(jnp.sum(total, axis=1, keepdims=True) * (1.0 / D) + EPSILON)
    for g in range(N_TP):
        x = in_ref[g].astype(F32) * scale * gain_ref[g, 0:1, :]
        x_ref[:, g * LANES : (g + 1) * LANES] = x.astype(BF16)
    hidden = []
    for g_ref, u_ref in ((g0_ref, u0_ref), (g1_ref, u1_ref)):
        gate = jnp.minimum(dot(x_ref[...], g_ref[...]), CLAMP_LIMIT)
        up = jnp.clip(dot(x_ref[...], u_ref[...]), -CLAMP_LIMIT, CLAMP_LIMIT)
        unit = gate * (1.0 / (1.0 + jnp.exp(-SIGMOID_SCALE * gate))) * (up + 1.0)
        hidden.append(unit.astype(BF16))
    for g in range(0, N_TP, 2):
        cols = slice(g * LANES, (g + 2) * LANES)
        part = dot(hidden[0], d0_ref[:, cols]) + dot(hidden[1], d1_ref[:, cols])
        part = part.astype(BF16)
        out_ref[g] = part[:, :LANES]
        out_ref[g + 1] = part[:, LANES:]


def gather_body(in_ref, widen_ref, out_ref):
    for c in range(2):
        total = in_ref[c].astype(F32)
        for y in range(1, N_Y):
            total = total + in_ref[y * 2 + c].astype(F32)
        rows = dot(widen_ref[...], total.astype(BF16)).astype(BF16)
        out_ref[c * 16 * CAP_PAD : (c + 1) * 16 * CAP_PAD, :] = rows


def finish_body(in_ref, mix_ref, mixed_ref, out_ref):
    total = mixed_ref[...]
    rows = in_ref[...]
    for i in range(3):
        total = total + dot(mix_ref[i].astype(BF16), rows, 0, 0)
    out_ref[...] = total.astype(BF16)


def shaped(shape, dtype=BF16):
    return jax.ShapeDtypeStruct(shape, dtype)


VMEM = pl.BlockSpec(memory_space=pltpu.VMEM)
SMEM = pl.BlockSpec(memory_space=pltpu.SMEM)


def call(body, outs, *args, scratch=(), name=None):
    specs = [SMEM if a.shape == (1,) else VMEM for a in args]
    many = isinstance(outs, (list, tuple))
    return pl.pallas_call(
        body,
        out_shape=outs,
        in_specs=specs,
        out_specs=[VMEM] * len(outs) if many else VMEM,
        scratch_shapes=list(scratch),
        name=name,
        compiler_params=pltpu.CompilerParams(vmem_limit_bytes=48 * 1024 * 1024),
    )(*args)


def exchange(x, axes):
    return lax.all_to_all(x, axes, 0, 0, tiled=True)


def partner(x):
    return lax.ppermute(x, "c", [(0, 1), (1, 0)])


def per_device(
    queries,
    keys,
    values,
    docs,
    query_gain,
    key_gain,
    out_weight,
    residual,
    norm_gain,
    routes,
    route_weight,
    gate_weight,
    up_weight,
    down_weight,
):
    row_tab, col_tab = tables()
    drop = compaction()
    block = (lax.axis_index("z") * N_X + lax.axis_index("x")).reshape(1).astype(jnp.int32)
    core = lax.axis_index("c").reshape(1).astype(jnp.int32)
    qs, kvs = call(
        prep_body,
        [shaped((N_X, TOK + NOTE, LANES)), shaped((N_Z, TOK + NOTE, LANES))],
        block,
        queries,
        keys.T,
        values.T,
        docs.reshape(2, LANES),
        query_gain.reshape(1, HD),
        key_gain.reshape(1, HD),
        jnp.asarray(row_tab),
        jnp.asarray(col_tab),
        name="prep",
    )
    kv_all = exchange(kvs, "z")
    q_all = exchange(qs, "x")
    gain_all = exchange(jnp.broadcast_to(norm_gain[None, None, :], (N_TP, 8, LANES)), ("y", "c"))
    gate, up, down = gate_weight[0], up_weight[0], down_weight[0]
    out_other = partner(out_weight)
    gate_o, up_o, down_o = partner(gate), partner(up), partner(down)
    place, mix = call(
        route_body,
        [shaped((EXPERTS * CAP_PAD, TOK), F32), shaped((3, EXPERTS * CAP_PAD, TOK), F32)],
        routes.T,
        route_weight.T,
        name="route",
    )
    partial = call(
        attend_body,
        shaped((N_X * 2, HALF + NOTE, LANES)),
        q_all,
        kv_all,
        scratch=[pltpu.VMEM((N_Z * TOK, LANES), BF16), pltpu.VMEM((N_Z * TOK, LANES), BF16)],
        name="attend",
    )
    partial = exchange(partial, ("x", "c"))
    projected = call(
        project_body,
        shaped((N_TP, HALF, LANES)),
        core,
        partial,
        out_weight,
        out_other,
        name="project",
    )
    projected = exchange(projected, ("y", "c"))
    mixed, outgoing = call(
        dispatch_body,
        [shaped((TOK, LANES), F32), shaped((EXPERTS * CAP_PAD, LANES))],
        projected,
        residual,
        place,
        name="dispatch",
    )
    arrived = exchange(outgoing.reshape(N_SP, CAP_PAD, LANES), ("z", "x"))
    spread = call(
        spread_body,
        shaped((N_TP, ROWS, LANES)),
        arrived.reshape(N_SP * CAP_PAD, LANES),
        jnp.asarray(drop, BF16),
        name="spread",
    )
    columns = exchange(spread, ("y", "c"))
    parts = call(
        expert_body,
        shaped((N_TP, ROWS, LANES)),
        columns,
        gain_all,
        gate,
        gate_o,
        up,
        up_o,
        down,
        down_o,
        scratch=[pltpu.VMEM((ROWS, D), BF16)],
        name="expert",
    )
    parts = exchange(parts, ("y", "c"))
    expert_out = call(
        gather_body,
        shaped((N_SP * CAP_PAD, LANES)),
        parts,
        jnp.asarray(drop.T, BF16),
        name="gather",
    )
    returned = exchange(expert_out.reshape(N_SP, CAP_PAD, LANES), ("z", "x"))
    return call(
        finish_body,
        shaped((TOK, LANES)),
        returned.reshape(N_SP * CAP_PAD, LANES),
        mix,
        mixed,
        name="finish",
    )


def solution(mesh):
    grid = Mesh(mesh.devices.reshape(N_Z, N_X, N_Y, N_C), ("z", "x", "y", "c"))
    sp, tp = ("z", "x"), ("y", "c")
    in_specs = (
        P(sp, tp),
        P(sp, tp),
        P(sp, tp),
        P(sp),
        P(),
        P(),
        P(tp, None),
        P(sp, tp),
        P(tp),
        P(sp, None),
        P(sp, None),
        P(sp, None, tp),
        P(sp, None, tp),
        P(sp, tp, None),
    )
    return jax.shard_map(
        per_device, mesh=grid, in_specs=in_specs, out_specs=P(sp, tp), check_vma=False
    )
```

```python
import functools

import jax
import jax.numpy as jnp
import numpy as np
from jax import lax
from jax.experimental import pallas as pl
from jax.experimental.pallas import tpu as pltpu
from jax.sharding import Mesh, PartitionSpec as P


GRID_W = 64
EPSILON = 1e-06
ROTARY_BASE = 10000.0
CLAMP_LIMIT = 7.0
SIGMOID_SCALE = 1.702
N_Z, N_X, N_Y, N_C = 8, 4, 8, 2
N_SP, N_TP = N_Z * N_X, N_Y * N_C
TOK = 256
HALF = TOK // 2
HD = 64
LANES = 128
D = 2048
EXPERTS = 32
CAP = 20
CAP_PAD = 24
PIECES = 1
ROWS = N_SP * CAP // (2 * PIECES)
BLOCKS = N_SP // (2 * PIECES)
NOTE = 16
MASK_BIG = 16384.0

F32 = jnp.float32
BF16 = jnp.bfloat16


def tables():
    quarter = HD // 4
    freqs = (ROTARY_BASE ** (-np.arange(quarter, dtype=np.float32) / quarter)).astype(np.float32)
    lane = np.arange(LANES)
    pair = (lane % HD) // 2
    is_row = pair < quarter
    freq = freqs[np.where(is_row, pair, pair - quarter)]
    sign = np.where(lane % 2 == 0, -1.0, 1.0)
    cols = (np.arange(GRID_W, dtype=np.float32)[:, None] * freq).astype(np.float32)
    rows = (np.arange(N_SP * TOK // GRID_W, dtype=np.float32)[:, None] * freq).astype(np.float32)
    cols, rows = cols.astype(np.float64), rows.astype(np.float64)
    keep = lambda a, m: np.where(m, a, 0.0).astype(np.float32)
    per = TOK // GRID_W
    row_c = keep(np.cos(rows), is_row).reshape(N_SP, per, LANES)
    row_s = keep(np.sin(rows) * sign, is_row).reshape(N_SP, per, LANES)
    row_tab = np.concatenate([row_c, row_s], axis=1)
    col_tab = np.stack([keep(np.cos(cols), ~is_row), keep(np.sin(cols) * sign, ~is_row)])
    return row_tab, col_tab


def compaction():
    out = np.zeros((ROWS, BLOCKS * CAP_PAD), np.float32)
    r = np.arange(ROWS)
    out[r, (r // CAP) * CAP_PAD + r % CAP] = 1.0
    return out


def dot(a, b, ca=1, cb=0):
    return lax.dot_general(a, b, (((ca,), (cb,)), ((), ())), preferred_element_type=F32)


def iota(shape, dim):
    return lax.broadcasted_iota(jnp.int32, shape, dim)


def prep_body(blk, *refs):
    sources, (qs_ref, kvs_ref), kept, sems = refs[:8], refs[8:10], refs[10:18], refs[18]
    copies = []
    for i, (src, dst) in enumerate(zip(sources, kept)):
        src = src.at[blk[0]] if i == 6 else src
        copies.append(pltpu.make_async_copy(src, dst, sems.at[i]))
    for copy in copies:
        copy.start()
    for copy in copies:
        copy.wait()
    q_ref, k_ref, v_ref, docs_ref, qg_ref, kg_ref, row_ref, col_ref = kept
    lane = iota((TOK, LANES), 1)
    low = lane < HD
    even = (lane & 1) == 0
    rows = row_ref[...]
    per = TOK // GRID_W
    cos_t = jnp.concatenate([col_ref[0] + rows[j : j + 1] for j in range(per)], axis=0)
    sin_t = jnp.concatenate([col_ref[1] + rows[per + j : per + j + 1] for j in range(per)], axis=0)

    def turn(n):
        swapped = jnp.where(even, pltpu.roll(n, LANES - 1, 1), pltpu.roll(n, 1, 1))
        return n * cos_t + swapped * sin_t

    x = q_ref[...].astype(F32)
    sq = x * x
    s0 = jnp.sum(jnp.where(low, sq, 0.0), axis=1, keepdims=True)
    s1 = jnp.sum(jnp.where(low, 0.0, sq), axis=1, keepdims=True)
    r0 = lax.rsqrt(s0 * (1.0 / HD) + EPSILON)
    r1 = lax.rsqrt(s1 * (1.0 / HD) + EPSILON)
    gain = jnp.concatenate([qg_ref[...], qg_ref[...]], axis=1)
    q_out = turn(x * jnp.where(low, r0, r1) * gain).astype(BF16)

    kv = jnp.concatenate([k_ref[...], v_ref[...]], axis=0).astype(F32).T
    sk = jnp.sum(jnp.where(low, kv * kv, 0.0), axis=1, keepdims=True)
    rk = lax.rsqrt(sk * (1.0 / HD) + EPSILON)
    gain_k = jnp.concatenate([kg_ref[...], kg_ref[...]], axis=1)
    kv_out = jnp.where(low, turn(kv * rk * gain_k), kv).astype(BF16)

    docs = docs_ref[...]
    n0 = jnp.sum((docs < 1).astype(F32))
    n1 = jnp.sum((docs < 2).astype(F32))
    row = iota((NOTE, LANES), 0)
    note = jnp.where(row == 0, n0, jnp.where(row == 1, n1, 0.0)).astype(BF16)
    qs_ref[:TOK, :] = q_out
    qs_ref[TOK:, :] = note
    for i in range(N_Z):
        kvs_ref[i, :TOK, :] = kv_out
        kvs_ref[i, TOK:, :] = note


def split3(x):
    hi = x.astype(BF16).astype(F32)
    mid = (x - hi).astype(BF16).astype(F32)
    return hi, mid, x - hi - mid


def attend_body(spot, *refs):
    q_refs, (kv_ref, out_ref, q_ref, kp_ref, vp_ref) = refs[:N_X], refs[N_X:]
    for i in range(N_X):
        q_ref[i] = q_refs[i][...]
    lane = iota((TOK, LANES), 1)
    low = lane < HD
    idx = iota((TOK, LANES), 0).astype(F32)

    def doc_of(note):
        n0 = note[0:1, :].astype(F32)
        n1 = note[1:2, :].astype(F32)
        return jnp.where(idx < n0, HD, jnp.where(idx < n1, HD + 1, HD + 2))

    for j in range(N_Z):
        kv = kv_ref[j, :TOK, :]
        mark = (doc_of(kv_ref[j, TOK:, :]) == lane).astype(F32)
        kvf = kv.astype(F32)
        kp_ref[j * TOK : (j + 1) * TOK, :] = jnp.where(low, kvf, mark).astype(BF16)
        vp_ref[j * TOK : (j + 1) * TOK, :] = jnp.where(low, 1.0, kvf).astype(BF16)
    eye = (iota((HALF, LANES), 0) == iota((HALF, LANES), 1)).astype(BF16)
    lane_h = iota((HALF, LANES), 1)

    def block(b, carry):
        qf = q_ref[b, :TOK, :].astype(F32) * (HD**-0.5)
        doc = doc_of(q_ref[b, TOK:, :])
        other = jnp.where((doc == lane) | (lane > HD + 2), 0.0, -MASK_BIG)
        heads = []
        for h in range(2):
            qh = qf if h == 0 else pltpu.roll(qf, HD, 1)
            qp = jnp.where(low, qh, other).astype(BF16)
            s = dot(qp, kp_ref[...], 1, 1)
            peak = jnp.max(s, axis=1, keepdims=True)
            p = jnp.exp(s - peak).astype(BF16)
            acc = dot(p, vp_ref[...])
            total = acc[:, 0:1]
            o = acc / total
            heads.append((pltpu.roll(o, HD, 1) if h == 0 else o, peak + jnp.log(total)))
        o = jnp.where(low, heads[0][0], heads[1][0]).astype(BF16)
        parts = split3(heads[0][1]) + split3(heads[1][1])
        for half in range(2):
            rows = slice(half * HALF, (half + 1) * HALF)
            stat = jnp.zeros((HALF, LANES), F32)
            for i, part in enumerate(parts):
                stat = jnp.where(lane_h == i, part[rows], stat)
            stat_t = dot(stat.astype(BF16), eye, 0, 0)
            to = lax.rem(spot[0] + N_X - b, N_X) * 2 + half
            out_ref[to, :HALF, :] = o[rows]
            out_ref[to, HALF:, :] = stat_t[:NOTE].astype(BF16)
        return carry

    lax.fori_loop(0, N_X, block, 0)


def project_body(core, in_ref, w_own_ref, w_other_ref, gain_ref, out_ref):
    gain = split3(gain_ref[...])
    row = iota((NOTE, LANES), 0)
    lane = iota((NOTE, LANES), 1)
    pick = (((row < 3) & (lane < HD)) | ((row >= 3) & (row < 6) & (lane >= HD))).astype(BF16)

    def attended(c):
        lse = [dot(in_ref[x * 2 + c, HALF:, :], pick, 0, 0) for x in range(N_X)]
        top = functools.reduce(jnp.maximum, lse)
        total = jnp.zeros((HALF, LANES), F32)
        mixed = jnp.zeros((HALF, LANES), F32)
        for x in range(N_X):
            w = jnp.exp(lse[x] - top)
            total = total + w
            mixed = mixed + w * in_ref[x * 2 + c, :HALF, :].astype(F32)
        return (mixed / total).astype(BF16)

    note = jnp.where(row == 0, gain[0], jnp.where(row == 1, gain[1], jnp.where(row == 2, gain[2], 0.0)))
    own = attended(core[0])
    other = attended(1 - core[0])
    for g in range(N_TP):
        cols = slice(g * LANES, (g + 1) * LANES)
        part = dot(own, w_own_ref[:, cols]) + dot(other, w_other_ref[:, cols])
        out_ref[g, :HALF, :] = part.astype(BF16)
        out_ref[g, HALF:, :] = note.astype(BF16)


def slots_of(routes_ref):
    expert = iota((EXPERTS, TOK), 0)
    r0, r1 = routes_ref[0:1, :], routes_ref[1:2, :]
    named = ((expert == r0) | (expert == r1)).astype(F32)
    before = (iota((TOK, TOK), 0) < iota((TOK, TOK), 1)).astype(BF16)
    slot = dot(named.astype(BF16), before)
    return expert == r0, expert == r1, jnp.where(named > 0.0, slot, -1.0)


def laid_out(slot, value, write):
    slots = iota((CAP_PAD, TOK), 0).astype(F32)
    for e in range(0, EXPERTS, 2):
        both = [jnp.where(slots == slot[i : i + 1, :], value(i), 0.0) for i in (e, e + 1)]
        write(slice(e * CAP_PAD, (e + 2) * CAP_PAD), jnp.concatenate(both, axis=0).astype(BF16))


def route_body(routes_ref, place_ref):
    _, _, slot = slots_of(routes_ref)

    def write(rows, value):
        place_ref[rows, :] = value

    laid_out(slot, lambda e: 1.0, write)


def mix_body(term, routes_ref, weight_ref, mix_ref):
    first, second, slot = slots_of(routes_ref)
    weight = jnp.where(first, weight_ref[0:1, :], jnp.where(second, weight_ref[1:2, :], 0.0))
    part = split3(weight)[term]

    def write(rows, value):
        mix_ref[rows, :] = value

    laid_out(slot, lambda e: part[e : e + 1, :], write)


def dispatch_body(in_ref, residual_ref, place_ref, mixed_ref, gain_ref, out_ref):
    halves = []
    for c in range(2):
        total = in_ref[c, :HALF, :].astype(F32)
        for y in range(1, N_Y):
            total = total + in_ref[y * 2 + c, :HALF, :].astype(F32)
        halves.append(total)
    for g in range(N_TP):
        note = in_ref[g, HALF:, :].astype(F32)
        gain = note[0:1] + note[1:2] + note[2:3]
        gain_ref[g] = jnp.broadcast_to(gain, (8, LANES))
    mixed = residual_ref[...].astype(F32) + jnp.concatenate(halves, axis=0)
    mixed_ref[...] = mixed
    out_ref[...] = dot(place_ref[...], mixed.astype(BF16)).astype(BF16)


def spread_body(in_ref, drop_ref, *out_refs):
    span = BLOCKS * CAP_PAD
    for c in range(2):
        for i, out_ref in enumerate(out_refs):
            at = (c * PIECES + i) * span
            kept = dot(drop_ref[...], in_ref[at : at + span, :]).astype(BF16)
            for y in range(N_Y):
                out_ref[y * 2 + c] = kept


def expert_body(in_ref, gain_ref, *refs):
    far, (out_ref, x_ref), weights, sems = refs[:6], refs[6:8], refs[8:14], refs[14]
    copies = [pltpu.make_async_copy(far[i], weights[i], sems.at[i]) for i in range(6)]
    for copy in copies:
        copy.start()
    total = jnp.zeros((ROWS, LANES), F32)
    for g in range(N_TP):
        x = in_ref[g].astype(F32)
        total = total + x * x
    scale = lax.rsqrt(jnp.sum(total, axis=1, keepdims=True) * (1.0 / D) + EPSILON)
    for g in range(N_TP):
        x = in_ref[g].astype(F32) * scale * gain_ref[g, 0:1, :]
        x_ref[:, g * LANES : (g + 1) * LANES] = x.astype(BF16)
    hidden = []
    for i in range(2):
        copies[2 * i].wait()
        gate = jnp.minimum(dot(x_ref[...], weights[2 * i][...]), CLAMP_LIMIT)
        copies[2 * i + 1].wait()
        up = jnp.clip(dot(x_ref[...], weights[2 * i + 1][...]), -CLAMP_LIMIT, CLAMP_LIMIT)
        unit = gate * (1.0 / (1.0 + jnp.exp(-SIGMOID_SCALE * gate))) * (up + 1.0)
        hidden.append(unit.astype(BF16))
    copies[4].wait()
    copies[5].wait()
    for g in range(0, N_TP, 2):
        cols = slice(g * LANES, (g + 2) * LANES)
        part = dot(hidden[0], weights[4][:, cols]) + dot(hidden[1], weights[5][:, cols])
        part = part.astype(BF16)
        out_ref[g] = part[:, :LANES]
        out_ref[g + 1] = part[:, LANES:]


def gather_body(*refs):
    in_refs, widen_ref, out_ref = refs[:PIECES], refs[PIECES], refs[PIECES + 1]
    span = BLOCKS * CAP_PAD
    for c in range(2):
        for i, in_ref in enumerate(in_refs):
            total = in_ref[c].astype(F32)
            for y in range(1, N_Y):
                total = total + in_ref[y * 2 + c].astype(F32)
            rows = dot(widen_ref[...], total.astype(BF16)).astype(BF16)
            at = (c * PIECES + i) * span
            out_ref[at : at + span, :] = rows


def finish_body(in_ref, mix0_ref, mix1_ref, mix2_ref, mixed_ref, out_ref):
    total = mixed_ref[...]
    rows = in_ref[...]
    for mix_ref in (mix0_ref, mix1_ref, mix2_ref):
        total = total + dot(mix_ref[...], rows, 0, 0)
    out_ref[...] = total.astype(BF16)


def shaped(shape, dtype=BF16):
    return jax.ShapeDtypeStruct(shape, dtype)


VMEM = pl.BlockSpec(memory_space=pltpu.VMEM)
SMEM = pl.BlockSpec(memory_space=pltpu.SMEM)
HBM = pl.BlockSpec(memory_space=pltpu.HBM)


def call(body, outs, *args, scratch=(), mib=8, far=0):
    near = len(args) - far
    specs = [SMEM if a.shape == (1,) else VMEM for a in args[:near]] + [HBM] * far
    args = args[:near] + tuple(pltpu.with_memory_space_constraint(a, pltpu.HBM) for a in args[near:])
    many = isinstance(outs, (list, tuple))
    return pl.pallas_call(
        body,
        out_shape=outs,
        in_specs=specs,
        out_specs=[VMEM] * len(outs) if many else VMEM,
        scratch_shapes=list(scratch),
        compiler_params=pltpu.CompilerParams(vmem_limit_bytes=mib * 1024 * 1024),
    )(*args)


def exchange(x, axes):
    return lax.all_to_all(x, axes, 0, 0, tiled=True)


def shifted(x, axis, size, by):
    return lax.ppermute(x, axis, [(i, (i + by) % size) for i in range(size)])


def partner(x):
    return lax.ppermute(x, "c", [(0, 1), (1, 0)])


def per_device(
    queries,
    keys,
    values,
    docs,
    query_gain,
    key_gain,
    out_weight,
    residual,
    norm_gain,
    routes,
    route_weight,
    gate_weight,
    up_weight,
    down_weight,
):
    return step(
        queries,
        keys.T,
        values.T,
        docs.reshape(2, LANES),
        query_gain.reshape(1, HD),
        key_gain.reshape(1, HD),
        out_weight,
        residual,
        norm_gain,
        routes.T,
        route_weight.T,
        gate_weight[0],
        up_weight[0],
        down_weight[0],
    )


def step(
    queries,
    keys,
    values,
    docs,
    query_gain,
    key_gain,
    out_weight,
    residual,
    norm_gain,
    routes,
    route_weight,
    gate,
    up,
    down,
):
    row_tab, col_tab = tables()
    drop = compaction()
    block = (lax.axis_index("z") * N_X + lax.axis_index("x")).reshape(1).astype(jnp.int32)
    spot = lax.axis_index("x").reshape(1).astype(jnp.int32)
    core = lax.axis_index("c").reshape(1).astype(jnp.int32)
    sources = (
        queries,
        keys,
        values,
        docs,
        query_gain,
        key_gain,
        jnp.asarray(row_tab),
        jnp.asarray(col_tab),
    )
    kept = [pltpu.VMEM(a.shape[1:] if i == 6 else a.shape, a.dtype) for i, a in enumerate(sources)]
    qs, kvs = call(
        prep_body,
        [shaped((TOK + NOTE, LANES)), shaped((N_Z, TOK + NOTE, LANES))],
        block,
        *sources,
        scratch=kept + [pltpu.SemaphoreType.DMA((len(sources),))],
        far=len(sources),
    )
    kv_all = exchange(kvs, "z")
    q_all = [qs] + [shifted(qs, "x", N_X, i) for i in range(1, N_X)]
    out_other = partner(out_weight)
    gate_o, up_o = partner(gate), partner(up)
    down_o = partner(down)
    slot_table = shaped((EXPERTS * CAP_PAD, TOK))
    place = call(route_body, slot_table, routes)
    mixes = [
        call(functools.partial(mix_body, i), slot_table, routes, route_weight)
        for i in range(3)
    ]
    partial = call(
        attend_body,
        shaped((N_X * 2, HALF + NOTE, LANES)),
        spot,
        *q_all,
        kv_all,
        scratch=[
            pltpu.VMEM((N_X, TOK + NOTE, LANES), BF16),
            pltpu.VMEM((N_Z * TOK, LANES), BF16),
            pltpu.VMEM((N_Z * TOK, LANES), BF16),
        ],
        mib=24,
    )
    partial = exchange(partial, ("x", "c"))
    projected = call(
        project_body,
        shaped((N_TP, HALF + NOTE, LANES)),
        core,
        partial,
        out_weight,
        out_other,
        norm_gain.reshape(1, LANES),
    )
    projected = exchange(projected, ("y", "c"))
    mixed, gain_all, outgoing = call(
        dispatch_body,
        [
            shaped((TOK, LANES), F32),
            shaped((N_TP, 8, LANES), F32),
            shaped((EXPERTS * CAP_PAD, LANES)),
        ],
        projected,
        residual,
        place,
    )
    arrived = exchange(outgoing.reshape(N_SP, CAP_PAD, LANES), ("z", "x"))
    pieces = call(
        spread_body,
        [shaped((N_TP, ROWS, LANES))] * PIECES,
        arrived.reshape(N_SP * CAP_PAD, LANES),
        jnp.asarray(drop, BF16),
    )
    pieces = [exchange(p, ("y", "c")) for p in pieces]
    weights = (gate, up, gate_o, up_o, down, down_o)
    parts = []
    for columns in pieces:
        part = call(
            expert_body,
            shaped((N_TP, ROWS, LANES)),
            columns,
            gain_all,
            *weights,
            scratch=[pltpu.VMEM((ROWS, D), BF16)]
            + [pltpu.VMEM(w.shape, BF16) for w in weights]
            + [pltpu.SemaphoreType.DMA((len(weights),))],
            mib=24,
            far=len(weights),
        )
        parts.append(exchange(part, ("y", "c")))
    expert_out = call(
        gather_body, shaped((N_SP * CAP_PAD, LANES)), *parts, jnp.asarray(drop.T, BF16)
    )
    returned = exchange(expert_out.reshape(N_SP, CAP_PAD, LANES), ("z", "x"))
    return call(
        finish_body, shaped((TOK, LANES)), returned.reshape(N_SP * CAP_PAD, LANES), *mixes, mixed
    )


def solution(mesh):
    grid = Mesh(mesh.devices.reshape(N_Z, N_X, N_Y, N_C), ("z", "x", "y", "c"))
    sp, tp = ("z", "x"), ("y", "c")
    in_specs = (
        P(sp, tp),
        P(sp, tp),
        P(sp, tp),
        P(sp),
        P(),
        P(),
        P(tp, None),
        P(sp, tp),
        P(tp),
        P(sp, None),
        P(sp, None),
        P(sp, None, tp),
        P(sp, None, tp),
        P(sp, tp, None),
    )
    return jax.shard_map(
        per_device, mesh=grid, in_specs=in_specs, out_specs=P(sp, tp), check_vma=False
    )
```

```python
import functools

import jax
import jax.numpy as jnp
import numpy as np
from jax import lax
from jax.experimental import pallas as pl
from jax.experimental.pallas import tpu as pltpu
from jax.sharding import Mesh, PartitionSpec as P


GRID_W = 64
EPSILON = 1e-06
ROTARY_BASE = 10000.0
CLAMP_LIMIT = 7.0
SIGMOID_SCALE = 1.702
N_Z, N_X, N_Y, N_C = 8, 4, 8, 2
N_SP, N_TP = N_Z * N_X, N_Y * N_C
TOK = 256
HALF = TOK // 2
HD = 64
LANES = 128
D = 2048
EXPERTS = 32
CAP = 20
CAP_PAD = 24
GROUPS = 4
ROWS = N_SP * CAP // GROUPS
BLOCKS = N_SP // GROUPS
NOTE = 16
MASK_BIG = 16384.0

F32 = jnp.float32
BF16 = jnp.bfloat16


def tables():
    quarter = HD // 4
    freqs = (ROTARY_BASE ** (-np.arange(quarter, dtype=np.float32) / quarter)).astype(np.float32)
    lane = np.arange(LANES)
    pair = (lane % HD) // 2
    is_row = pair < quarter
    freq = freqs[np.where(is_row, pair, pair - quarter)]
    sign = np.where(lane % 2 == 0, -1.0, 1.0)
    cols = (np.arange(GRID_W, dtype=np.float32)[:, None] * freq).astype(np.float32)
    rows = (np.arange(N_SP * TOK // GRID_W, dtype=np.float32)[:, None] * freq).astype(np.float32)
    cols, rows = cols.astype(np.float64), rows.astype(np.float64)
    keep = lambda a, m: np.where(m, a, 0.0).astype(np.float32)
    per = TOK // GRID_W
    row_c = keep(np.cos(rows), is_row).reshape(N_SP, per, LANES)
    row_s = keep(np.sin(rows) * sign, is_row).reshape(N_SP, per, LANES)
    row_tab = np.concatenate([row_c, row_s], axis=1)
    col_tab = np.stack([keep(np.cos(cols), ~is_row), keep(np.sin(cols) * sign, ~is_row)])
    return row_tab, col_tab


def compaction():
    out = np.zeros((ROWS, BLOCKS * CAP_PAD), np.float32)
    r = np.arange(ROWS)
    out[r, (r // CAP) * CAP_PAD + r % CAP] = 1.0
    return out


def dot(a, b, ca=1, cb=0):
    return lax.dot_general(a, b, (((ca,), (cb,)), ((), ())), preferred_element_type=F32)


def iota(shape, dim):
    return lax.broadcasted_iota(jnp.int32, shape, dim)


def prep_body(blk, *refs):
    sources, (qs_ref, kvs_ref), kept, sems = refs[:8], refs[8:10], refs[10:18], refs[18]
    copies = []
    for i, (src, dst) in enumerate(zip(sources, kept)):
        src = src.at[blk[0]] if i == 6 else src
        copies.append(pltpu.make_async_copy(src, dst, sems.at[i]))
    for copy in copies:
        copy.start()
    for copy in copies:
        copy.wait()
    q_ref, k_ref, v_ref, docs_ref, qg_ref, kg_ref, row_ref, col_ref = kept
    lane = iota((TOK, LANES), 1)
    low = lane < HD
    even = (lane & 1) == 0
    rows = row_ref[...]
    per = TOK // GRID_W
    cos_t = jnp.concatenate([col_ref[0] + rows[j : j + 1] for j in range(per)], axis=0)
    sin_t = jnp.concatenate([col_ref[1] + rows[per + j : per + j + 1] for j in range(per)], axis=0)

    def turn(n):
        swapped = jnp.where(even, pltpu.roll(n, LANES - 1, 1), pltpu.roll(n, 1, 1))
        return n * cos_t + swapped * sin_t

    x = q_ref[...].astype(F32)
    sq = x * x
    s0 = jnp.sum(jnp.where(low, sq, 0.0), axis=1, keepdims=True)
    s1 = jnp.sum(jnp.where(low, 0.0, sq), axis=1, keepdims=True)
    r0 = lax.rsqrt(s0 * (1.0 / HD) + EPSILON)
    r1 = lax.rsqrt(s1 * (1.0 / HD) + EPSILON)
    gain = jnp.concatenate([qg_ref[...], qg_ref[...]], axis=1)
    q_out = turn(x * jnp.where(low, r0, r1) * gain).astype(BF16)

    kv = jnp.concatenate([k_ref[...], v_ref[...]], axis=0).astype(F32).T
    sk = jnp.sum(jnp.where(low, kv * kv, 0.0), axis=1, keepdims=True)
    rk = lax.rsqrt(sk * (1.0 / HD) + EPSILON)
    gain_k = jnp.concatenate([kg_ref[...], kg_ref[...]], axis=1)
    kv_out = jnp.where(low, turn(kv * rk * gain_k), kv).astype(BF16)

    docs = docs_ref[...]
    n0 = jnp.sum((docs < 1).astype(F32))
    n1 = jnp.sum((docs < 2).astype(F32))
    row = iota((NOTE, LANES), 0)
    note = jnp.where(row == 0, n0, jnp.where(row == 1, n1, 0.0)).astype(BF16)
    qs_ref[:TOK, :] = q_out
    qs_ref[TOK:, :] = note
    for i in range(N_Z):
        kvs_ref[i, :TOK, :] = kv_out
        kvs_ref[i, TOK:, :] = note


def split3(x):
    hi = x.astype(BF16).astype(F32)
    mid = (x - hi).astype(BF16).astype(F32)
    return hi, mid, x - hi - mid


def attend_body(spot, *refs):
    q_refs, (kv_ref, out_ref, q_ref, kp_ref, vp_ref) = refs[:N_X], refs[N_X:]
    for i in range(N_X):
        q_ref[i] = q_refs[i][...]
    lane = iota((TOK, LANES), 1)
    low = lane < HD
    idx = iota((TOK, LANES), 0).astype(F32)

    def doc_of(note):
        n0 = note[0:1, :].astype(F32)
        n1 = note[1:2, :].astype(F32)
        return jnp.where(idx < n0, HD, jnp.where(idx < n1, HD + 1, HD + 2))

    for j in range(N_Z):
        kv = kv_ref[j, :TOK, :]
        mark = (doc_of(kv_ref[j, TOK:, :]) == lane).astype(F32)
        kvf = kv.astype(F32)
        kp_ref[j * TOK : (j + 1) * TOK, :] = jnp.where(low, kvf, mark).astype(BF16)
        vp_ref[j * TOK : (j + 1) * TOK, :] = jnp.where(low, 1.0, kvf).astype(BF16)
    eye = (iota((HALF, LANES), 0) == iota((HALF, LANES), 1)).astype(BF16)
    lane_h = iota((HALF, LANES), 1)

    def block(b, carry):
        qf = q_ref[b, :TOK, :].astype(F32) * (HD**-0.5)
        doc = doc_of(q_ref[b, TOK:, :])
        other = jnp.where((doc == lane) | (lane > HD + 2), 0.0, -MASK_BIG)
        heads = []
        for h in range(2):
            qh = qf if h == 0 else pltpu.roll(qf, HD, 1)
            qp = jnp.where(low, qh, other).astype(BF16)
            s = dot(qp, kp_ref[...], 1, 1)
            peak = jnp.max(s, axis=1, keepdims=True)
            p = jnp.exp(s - peak).astype(BF16)
            acc = dot(p, vp_ref[...])
            total = acc[:, 0:1]
            o = acc / total
            heads.append((pltpu.roll(o, HD, 1) if h == 0 else o, peak + jnp.log(total)))
        o = jnp.where(low, heads[0][0], heads[1][0]).astype(BF16)
        parts = split3(heads[0][1]) + split3(heads[1][1])
        for half in range(2):
            rows = slice(half * HALF, (half + 1) * HALF)
            stat = jnp.zeros((HALF, LANES), F32)
            for i, part in enumerate(parts):
                stat = jnp.where(lane_h == i, part[rows], stat)
            stat_t = dot(stat.astype(BF16), eye, 0, 0)
            to = lax.rem(spot[0] + N_X - b, N_X) * 2 + half
            out_ref[to, :HALF, :] = o[rows]
            out_ref[to, HALF:, :] = stat_t[:NOTE].astype(BF16)
        return carry

    lax.fori_loop(0, N_X, block, 0)


def project_body(core, in_ref, w_own_ref, w_other_ref, gain_ref, out_ref):
    gain = split3(gain_ref[...])
    row = iota((NOTE, LANES), 0)
    lane = iota((NOTE, LANES), 1)
    pick = (((row < 3) & (lane < HD)) | ((row >= 3) & (row < 6) & (lane >= HD))).astype(BF16)

    def attended(c):
        lse = [dot(in_ref[x * 2 + c, HALF:, :], pick, 0, 0) for x in range(N_X)]
        top = functools.reduce(jnp.maximum, lse)
        total = jnp.zeros((HALF, LANES), F32)
        mixed = jnp.zeros((HALF, LANES), F32)
        for x in range(N_X):
            w = jnp.exp(lse[x] - top)
            total = total + w
            mixed = mixed + w * in_ref[x * 2 + c, :HALF, :].astype(F32)
        return (mixed / total).astype(BF16)

    note = jnp.where(row == 0, gain[0], jnp.where(row == 1, gain[1], jnp.where(row == 2, gain[2], 0.0)))
    own = attended(core[0])
    other = attended(1 - core[0])
    for g in range(N_TP):
        cols = slice(g * LANES, (g + 1) * LANES)
        part = dot(own, w_own_ref[:, cols]) + dot(other, w_other_ref[:, cols])
        out_ref[g, :HALF, :] = part.astype(BF16)
        out_ref[g, HALF:, :] = note.astype(BF16)


def slots_of(routes_ref):
    expert = iota((EXPERTS, TOK), 0)
    r0, r1 = routes_ref[0:1, :], routes_ref[1:2, :]
    named = ((expert == r0) | (expert == r1)).astype(F32)
    before = (iota((TOK, TOK), 0) < iota((TOK, TOK), 1)).astype(BF16)
    slot = dot(named.astype(BF16), before)
    return expert == r0, expert == r1, jnp.where(named > 0.0, slot, -1.0)


def laid_out(slot, value, write):
    slots = iota((CAP_PAD, TOK), 0).astype(F32)
    for e in range(0, EXPERTS, 2):
        both = [jnp.where(slots == slot[i : i + 1, :], value(i), 0.0) for i in (e, e + 1)]
        write(slice(e * CAP_PAD, (e + 2) * CAP_PAD), jnp.concatenate(both, axis=0).astype(BF16))


def route_body(routes_ref, place_ref):
    _, _, slot = slots_of(routes_ref)

    def write(rows, value):
        place_ref[rows, :] = value

    laid_out(slot, lambda e: 1.0, write)


def mix_body(term, routes_ref, weight_ref, mix_ref):
    first, second, slot = slots_of(routes_ref)
    weight = jnp.where(first, weight_ref[0:1, :], jnp.where(second, weight_ref[1:2, :], 0.0))
    part = split3(weight)[term]

    def write(rows, value):
        mix_ref[rows, :] = value

    laid_out(slot, lambda e: part[e : e + 1, :], write)


def dispatch_body(in_ref, residual_ref, place_ref, mixed_ref, gain_ref, out_ref):
    halves = []
    for c in range(2):
        total = in_ref[c, :HALF, :].astype(F32)
        for y in range(1, N_Y):
            total = total + in_ref[y * 2 + c, :HALF, :].astype(F32)
        halves.append(total)
    for g in range(N_TP):
        note = in_ref[g, HALF:, :].astype(F32)
        gain = note[0:1] + note[1:2] + note[2:3]
        gain_ref[g] = jnp.broadcast_to(gain, (8, LANES))
    mixed = residual_ref[...].astype(F32) + jnp.concatenate(halves, axis=0)
    mixed_ref[...] = mixed
    out_ref[...] = dot(place_ref[...], mixed.astype(BF16)).astype(BF16)


def spread_body(in_ref, drop_ref, out_ref):
    span = BLOCKS * CAP_PAD
    for r in range(GROUPS):
        kept = dot(drop_ref[...], in_ref[r * span : (r + 1) * span, :]).astype(BF16)
        for g in range(r, N_TP, GROUPS):
            out_ref[g] = kept


def expert_body(in_ref, gain_ref, *refs):
    many = 3 * GROUPS
    far, (out_ref, x_ref), weights, sems = refs[:many], refs[many : many + 2], refs[many + 2 : -1], refs[-1]
    copies = [pltpu.make_async_copy(far[i], weights[i], sems.at[i]) for i in range(many)]
    for copy in copies:
        copy.start()
    total = jnp.zeros((ROWS, LANES), F32)
    for g in range(N_TP):
        x = in_ref[g].astype(F32)
        total = total + x * x
    scale = lax.rsqrt(jnp.sum(total, axis=1, keepdims=True) * (1.0 / D) + EPSILON)
    for g in range(N_TP):
        x = in_ref[g].astype(F32) * scale * gain_ref[g, 0:1, :]
        x_ref[:, g * LANES : (g + 1) * LANES] = x.astype(BF16)
    hidden = []
    for i in range(GROUPS):
        copies[2 * i].wait()
        gate = jnp.minimum(dot(x_ref[...], weights[2 * i][...]), CLAMP_LIMIT)
        copies[2 * i + 1].wait()
        up = jnp.clip(dot(x_ref[...], weights[2 * i + 1][...]), -CLAMP_LIMIT, CLAMP_LIMIT)
        unit = gate * (1.0 / (1.0 + jnp.exp(-SIGMOID_SCALE * gate))) * (up + 1.0)
        hidden.append(unit.astype(BF16))
    for copy in copies[2 * GROUPS :]:
        copy.wait()
    downs = weights[2 * GROUPS :]
    for g in range(0, N_TP, 2):
        cols = slice(g * LANES, (g + 2) * LANES)
        part = dot(hidden[0], downs[0][:, cols])
        for h, w in zip(hidden[1:], downs[1:]):
            part = part + dot(h, w[:, cols])
        part = part.astype(BF16)
        out_ref[g] = part[:, :LANES]
        out_ref[g + 1] = part[:, LANES:]


def gather_body(in_ref, widen_ref, out_ref):
    span = BLOCKS * CAP_PAD
    for r in range(GROUPS):
        total = in_ref[r].astype(F32)
        for g in range(r + GROUPS, N_TP, GROUPS):
            total = total + in_ref[g].astype(F32)
        rows = dot(widen_ref[...], total.astype(BF16)).astype(BF16)
        out_ref[r * span : (r + 1) * span, :] = rows


def finish_body(in_ref, mix0_ref, mix1_ref, mix2_ref, mixed_ref, out_ref):
    total = mixed_ref[...]
    rows = in_ref[...]
    for mix_ref in (mix0_ref, mix1_ref, mix2_ref):
        total = total + dot(mix_ref[...], rows, 0, 0)
    out_ref[...] = total.astype(BF16)


def shaped(shape, dtype=BF16):
    return jax.ShapeDtypeStruct(shape, dtype)


VMEM = pl.BlockSpec(memory_space=pltpu.VMEM)
SMEM = pl.BlockSpec(memory_space=pltpu.SMEM)
HBM = pl.BlockSpec(memory_space=pltpu.HBM)


def call(body, outs, *args, scratch=(), mib=8, far=0):
    near = len(args) - far
    specs = [SMEM if a.shape == (1,) else VMEM for a in args[:near]] + [HBM] * far
    args = args[:near] + tuple(pltpu.with_memory_space_constraint(a, pltpu.HBM) for a in args[near:])
    many = isinstance(outs, (list, tuple))
    return pl.pallas_call(
        body,
        out_shape=outs,
        in_specs=specs,
        out_specs=[VMEM] * len(outs) if many else VMEM,
        scratch_shapes=list(scratch),
        compiler_params=pltpu.CompilerParams(vmem_limit_bytes=mib * 1024 * 1024),
    )(*args)


def exchange(x, axes):
    return lax.all_to_all(x, axes, 0, 0, tiled=True)


def shifted(x, axis, size, by):
    return lax.ppermute(x, axis, [(i, (i + by) % size) for i in range(size)])


def partner(x):
    return lax.ppermute(x, "c", [(0, 1), (1, 0)])


def neighbour(x):
    return lax.ppermute(x, "y", [(i, i ^ 1) for i in range(N_Y)])


def per_device(
    queries,
    keys,
    values,
    docs,
    query_gain,
    key_gain,
    out_weight,
    residual,
    norm_gain,
    routes,
    route_weight,
    gate_weight,
    up_weight,
    down_weight,
):
    return step(
        queries,
        keys.T,
        values.T,
        docs.reshape(2, LANES),
        query_gain.reshape(1, HD),
        key_gain.reshape(1, HD),
        out_weight,
        residual,
        norm_gain,
        routes.T,
        route_weight.T,
        gate_weight[0],
        up_weight[0],
        down_weight[0],
    )


def step(
    queries,
    keys,
    values,
    docs,
    query_gain,
    key_gain,
    out_weight,
    residual,
    norm_gain,
    routes,
    route_weight,
    gate,
    up,
    down,
):
    row_tab, col_tab = tables()
    drop = compaction()
    block = (lax.axis_index("z") * N_X + lax.axis_index("x")).reshape(1).astype(jnp.int32)
    spot = lax.axis_index("x").reshape(1).astype(jnp.int32)
    core = lax.axis_index("c").reshape(1).astype(jnp.int32)
    sources = (
        queries,
        keys,
        values,
        docs,
        query_gain,
        key_gain,
        jnp.asarray(row_tab),
        jnp.asarray(col_tab),
    )
    kept = [pltpu.VMEM(a.shape[1:] if i == 6 else a.shape, a.dtype) for i, a in enumerate(sources)]
    qs, kvs = call(
        prep_body,
        [shaped((TOK + NOTE, LANES)), shaped((N_Z, TOK + NOTE, LANES))],
        block,
        *sources,
        scratch=kept + [pltpu.SemaphoreType.DMA((len(sources),))],
        far=len(sources),
    )
    kv_all = exchange(kvs, "z")
    q_all = [qs] + [shifted(qs, "x", N_X, i) for i in range(1, N_X)]
    out_other = partner(out_weight)
    gate_y, up_y = neighbour(gate), neighbour(up)
    down_y = neighbour(down)
    gate_o, up_o = partner(gate), partner(up)
    down_o = partner(down)
    gate_yo, up_yo = partner(gate_y), partner(up_y)
    down_yo = partner(down_y)
    slot_table = shaped((EXPERTS * CAP_PAD, TOK))
    place = call(route_body, slot_table, routes)
    mixes = [
        call(functools.partial(mix_body, i), slot_table, routes, route_weight)
        for i in range(3)
    ]
    partial = call(
        attend_body,
        shaped((N_X * 2, HALF + NOTE, LANES)),
        spot,
        *q_all,
        kv_all,
        scratch=[
            pltpu.VMEM((N_X, TOK + NOTE, LANES), BF16),
            pltpu.VMEM((N_Z * TOK, LANES), BF16),
            pltpu.VMEM((N_Z * TOK, LANES), BF16),
        ],
        mib=24,
    )
    partial = exchange(partial, ("x", "c"))
    projected = call(
        project_body,
        shaped((N_TP, HALF + NOTE, LANES)),
        core,
        partial,
        out_weight,
        out_other,
        norm_gain.reshape(1, LANES),
    )
    projected = exchange(projected, ("y", "c"))
    mixed, gain_all, outgoing = call(
        dispatch_body,
        [
            shaped((TOK, LANES), F32),
            shaped((N_TP, 8, LANES), F32),
            shaped((EXPERTS * CAP_PAD, LANES)),
        ],
        projected,
        residual,
        place,
    )
    arrived = exchange(outgoing.reshape(N_SP, CAP_PAD, LANES), ("z", "x"))
    spread = call(
        spread_body,
        shaped((N_TP, ROWS, LANES)),
        arrived.reshape(N_SP * CAP_PAD, LANES),
        jnp.asarray(drop, BF16),
    )
    columns = exchange(spread, ("y", "c"))
    weights = (gate, up, gate_o, up_o, gate_y, up_y, gate_yo, up_yo, down, down_o, down_y, down_yo)
    parts = call(
        expert_body,
        shaped((N_TP, ROWS, LANES)),
        columns,
        gain_all,
        *weights,
        scratch=[pltpu.VMEM((ROWS, D), BF16)]
        + [pltpu.VMEM(w.shape, BF16) for w in weights]
        + [pltpu.SemaphoreType.DMA((len(weights),))],
        mib=32,
        far=len(weights),
    )
    parts = exchange(parts, ("y", "c"))
    expert_out = call(
        gather_body, shaped((N_SP * CAP_PAD, LANES)), parts, jnp.asarray(drop.T, BF16)
    )
    returned = exchange(expert_out.reshape(N_SP, CAP_PAD, LANES), ("z", "x"))
    return call(
        finish_body, shaped((TOK, LANES)), returned.reshape(N_SP * CAP_PAD, LANES), *mixes, mixed
    )


def solution(mesh):
    grid = Mesh(mesh.devices.reshape(N_Z, N_X, N_Y, N_C), ("z", "x", "y", "c"))
    sp, tp = ("z", "x"), ("y", "c")
    in_specs = (
        P(sp, tp),
        P(sp, tp),
        P(sp, tp),
        P(sp),
        P(),
        P(),
        P(tp, None),
        P(sp, tp),
        P(tp),
        P(sp, None),
        P(sp, None),
        P(sp, None, tp),
        P(sp, None, tp),
        P(sp, tp, None),
    )
    return jax.shard_map(
        per_device, mesh=grid, in_specs=in_specs, out_specs=P(sp, tp), check_vma=False
    )
```

```python
import functools

import jax
import jax.numpy as jnp
import numpy as np
from jax import lax
from jax.experimental import pallas as pl
from jax.experimental.pallas import tpu as pltpu
from jax.sharding import Mesh, PartitionSpec as P


GRID_W = 64
EPSILON = 1e-06
ROTARY_BASE = 10000.0
CLAMP_LIMIT = 7.0
SIGMOID_SCALE = 1.702
N_Z, N_X, N_Y, N_C = 8, 4, 8, 2
N_SP, N_TP = N_Z * N_X, N_Y * N_C
TOK = 256
HALF = TOK // 2
HD = 64
LANES = 128
D = 2048
EXPERTS = 32
CAP = 20
CAP_PAD = 24
GROUPS = 4
ROWS = N_SP * CAP // GROUPS
BLOCKS = N_SP // GROUPS
NOTE = 16
MASK_BIG = 16384.0

F32 = jnp.float32
BF16 = jnp.bfloat16


def tables():
    quarter = HD // 4
    freqs = (ROTARY_BASE ** (-np.arange(quarter, dtype=np.float32) / quarter)).astype(np.float32)
    lane = np.arange(LANES)
    pair = (lane % HD) // 2
    is_row = pair < quarter
    freq = freqs[np.where(is_row, pair, pair - quarter)]
    sign = np.where(lane % 2 == 0, -1.0, 1.0)
    cols = (np.arange(GRID_W, dtype=np.float32)[:, None] * freq).astype(np.float32)
    rows = (np.arange(N_SP * TOK // GRID_W, dtype=np.float32)[:, None] * freq).astype(np.float32)
    cols, rows = cols.astype(np.float64), rows.astype(np.float64)
    keep = lambda a, m: np.where(m, a, 0.0).astype(np.float32)
    per = TOK // GRID_W
    row_c = keep(np.cos(rows), is_row).reshape(N_SP, per, LANES)
    row_s = keep(np.sin(rows) * sign, is_row).reshape(N_SP, per, LANES)
    row_tab = np.concatenate([row_c, row_s], axis=1)
    col_tab = np.stack([keep(np.cos(cols), ~is_row), keep(np.sin(cols) * sign, ~is_row)])
    return row_tab, col_tab


def compaction():
    out = np.zeros((ROWS, BLOCKS * CAP_PAD), np.float32)
    r = np.arange(ROWS)
    out[r, (r // CAP) * CAP_PAD + r % CAP] = 1.0
    return out


def dot(a, b, ca=1, cb=0):
    return lax.dot_general(a, b, (((ca,), (cb,)), ((), ())), preferred_element_type=F32)


def iota(shape, dim):
    return lax.broadcasted_iota(jnp.int32, shape, dim)


def prep_body(blk, *refs):
    sources, (qs_ref, kvs_ref), kept, sems = refs[:8], refs[8:10], refs[10:18], refs[18]
    copies = []
    for i, (src, dst) in enumerate(zip(sources, kept)):
        src = src.at[blk[0]] if i == 6 else src
        copies.append(pltpu.make_async_copy(src, dst, sems.at[i]))
    for copy in copies:
        copy.start()
    for copy in copies:
        copy.wait()
    q_ref, k_ref, v_ref, docs_ref, qg_ref, kg_ref, row_ref, col_ref = kept
    lane = iota((TOK, LANES), 1)
    low = lane < HD
    even = (lane & 1) == 0
    rows = row_ref[...]
    per = TOK // GRID_W
    cos_t = jnp.concatenate([col_ref[0] + rows[j : j + 1] for j in range(per)], axis=0)
    sin_t = jnp.concatenate([col_ref[1] + rows[per + j : per + j + 1] for j in range(per)], axis=0)

    def turn(n):
        swapped = jnp.where(even, pltpu.roll(n, LANES - 1, 1), pltpu.roll(n, 1, 1))
        return n * cos_t + swapped * sin_t

    x = q_ref[...].astype(F32)
    sq = x * x
    s0 = jnp.sum(jnp.where(low, sq, 0.0), axis=1, keepdims=True)
    s1 = jnp.sum(jnp.where(low, 0.0, sq), axis=1, keepdims=True)
    r0 = lax.rsqrt(s0 * (1.0 / HD) + EPSILON)
    r1 = lax.rsqrt(s1 * (1.0 / HD) + EPSILON)
    gain = jnp.concatenate([qg_ref[...], qg_ref[...]], axis=1)
    q_out = turn(x * jnp.where(low, r0, r1) * gain).astype(BF16)

    kv = jnp.concatenate([k_ref[...], v_ref[...]], axis=0).astype(F32).T
    sk = jnp.sum(jnp.where(low, kv * kv, 0.0), axis=1, keepdims=True)
    rk = lax.rsqrt(sk * (1.0 / HD) + EPSILON)
    gain_k = jnp.concatenate([kg_ref[...], kg_ref[...]], axis=1)
    kv_out = jnp.where(low, turn(kv * rk * gain_k), kv).astype(BF16)

    docs = docs_ref[...]
    n0 = jnp.sum((docs < 1).astype(F32))
    n1 = jnp.sum((docs < 2).astype(F32))
    row = iota((NOTE, LANES), 0)
    note = jnp.where(row == 0, n0, jnp.where(row == 1, n1, 0.0)).astype(BF16)
    qs_ref[:TOK, :] = q_out
    qs_ref[TOK:, :] = note
    for i in range(N_Z):
        kvs_ref[i, :TOK, :] = kv_out
        kvs_ref[i, TOK:, :] = note


def split3(x):
    hi = x.astype(BF16).astype(F32)
    mid = (x - hi).astype(BF16).astype(F32)
    return hi, mid, x - hi - mid


def attend_body(spot, *refs):
    q_refs, (kv_ref, out_ref, q_ref, kp_ref, vp_ref) = refs[:N_X], refs[N_X:]
    for i in range(N_X):
        q_ref[i] = q_refs[i][...]
    lane = iota((TOK, LANES), 1)
    low = lane < HD
    idx = iota((TOK, LANES), 0).astype(F32)

    def doc_of(note):
        n0 = note[0:1, :].astype(F32)
        n1 = note[1:2, :].astype(F32)
        return jnp.where(idx < n0, HD, jnp.where(idx < n1, HD + 1, HD + 2))

    for j in range(N_Z):
        kv = kv_ref[j, :TOK, :]
        mark = (doc_of(kv_ref[j, TOK:, :]) == lane).astype(F32)
        kvf = kv.astype(F32)
        kp_ref[j * TOK : (j + 1) * TOK, :] = jnp.where(low, kvf, mark).astype(BF16)
        vp_ref[j * TOK : (j + 1) * TOK, :] = jnp.where(low, 1.0, kvf).astype(BF16)
    eye = (iota((HALF, LANES), 0) == iota((HALF, LANES), 1)).astype(BF16)
    lane_h = iota((HALF, LANES), 1)

    def block(b, carry):
        qf = q_ref[b, :TOK, :].astype(F32) * (HD**-0.5)
        doc = doc_of(q_ref[b, TOK:, :])
        other = jnp.where((doc == lane) | (lane > HD + 2), 0.0, -MASK_BIG)
        heads = []
        for h in range(2):
            qh = qf if h == 0 else pltpu.roll(qf, HD, 1)
            qp = jnp.where(low, qh, other).astype(BF16)
            s = dot(qp, kp_ref[...], 1, 1)
            peak = jnp.max(s, axis=1, keepdims=True)
            p = jnp.exp(s - peak).astype(BF16)
            acc = dot(p, vp_ref[...])
            total = acc[:, 0:1]
            o = acc / total
            heads.append((pltpu.roll(o, HD, 1) if h == 0 else o, peak + jnp.log(total)))
        o = jnp.where(low, heads[0][0], heads[1][0]).astype(BF16)
        parts = split3(heads[0][1]) + split3(heads[1][1])
        for half in range(2):
            rows = slice(half * HALF, (half + 1) * HALF)
            stat = jnp.zeros((HALF, LANES), F32)
            for i, part in enumerate(parts):
                stat = jnp.where(lane_h == i, part[rows], stat)
            stat_t = dot(stat.astype(BF16), eye, 0, 0)
            to = lax.rem(spot[0] + N_X - b, N_X) * 2 + half
            out_ref[to, :HALF, :] = o[rows]
            out_ref[to, HALF:, :] = stat_t[:NOTE].astype(BF16)
        return carry

    lax.fori_loop(0, N_X, block, 0)


def project_body(core, in_ref, w_own_ref, w_other_ref, gain_ref, out_ref):
    gain = split3(gain_ref[...])
    row = iota((NOTE, LANES), 0)
    lane = iota((NOTE, LANES), 1)
    pick = (((row < 3) & (lane < HD)) | ((row >= 3) & (row < 6) & (lane >= HD))).astype(BF16)

    def attended(c):
        lse = [dot(in_ref[x * 2 + c, HALF:, :], pick, 0, 0) for x in range(N_X)]
        top = functools.reduce(jnp.maximum, lse)
        total = jnp.zeros((HALF, LANES), F32)
        mixed = jnp.zeros((HALF, LANES), F32)
        for x in range(N_X):
            w = jnp.exp(lse[x] - top)
            total = total + w
            mixed = mixed + w * in_ref[x * 2 + c, :HALF, :].astype(F32)
        return (mixed / total).astype(BF16)

    note = jnp.where(row == 0, gain[0], jnp.where(row == 1, gain[1], jnp.where(row == 2, gain[2], 0.0)))
    own = attended(core[0])
    other = attended(1 - core[0])
    for g in range(N_TP):
        cols = slice(g * LANES, (g + 1) * LANES)
        part = dot(own, w_own_ref[:, cols]) + dot(other, w_other_ref[:, cols])
        out_ref[g, :HALF, :] = part.astype(BF16)
        out_ref[g, HALF:, :] = note.astype(BF16)


def slots_of(routes_ref):
    expert = iota((EXPERTS, TOK), 0)
    r0, r1 = routes_ref[0:1, :], routes_ref[1:2, :]
    named = ((expert == r0) | (expert == r1)).astype(F32)
    before = (iota((TOK, TOK), 0) < iota((TOK, TOK), 1)).astype(BF16)
    slot = dot(named.astype(BF16), before)
    return expert == r0, expert == r1, jnp.where(named > 0.0, slot, -1.0)


def laid_out(slot, value, write):
    slots = iota((CAP_PAD, TOK), 0).astype(F32)
    for e in range(0, EXPERTS, 2):
        both = [jnp.where(slots == slot[i : i + 1, :], value(i), 0.0) for i in (e, e + 1)]
        write(slice(e * CAP_PAD, (e + 2) * CAP_PAD), jnp.concatenate(both, axis=0).astype(BF16))


def route_body(routes_ref, place_ref):
    _, _, slot = slots_of(routes_ref)

    def write(rows, value):
        place_ref[rows, :] = value

    laid_out(slot, lambda e: 1.0, write)


def mix_body(term, routes_ref, weight_ref, mix_ref):
    first, second, slot = slots_of(routes_ref)
    weight = jnp.where(first, weight_ref[0:1, :], jnp.where(second, weight_ref[1:2, :], 0.0))
    part = split3(weight)[term]

    parts = []
    laid_out(slot, lambda e: part[e : e + 1, :], lambda rows, value: parts.append(value))
    for i in range(0, len(parts), 8):
        some = jnp.concatenate(parts[i : i + 8], axis=0).astype(F32)
        mix_ref[:, i * 2 * CAP_PAD : (i + 8) * 2 * CAP_PAD] = some.T.astype(BF16)


def dispatch_body(in_ref, residual_ref, place_ref, mixed_ref, gain_ref, out_ref):
    halves = []
    for c in range(2):
        total = in_ref[c, :HALF, :].astype(F32)
        for y in range(1, N_Y):
            total = total + in_ref[y * 2 + c, :HALF, :].astype(F32)
        halves.append(total)
    for g in range(N_TP):
        note = in_ref[g, HALF:, :].astype(F32)
        gain = note[0:1] + note[1:2] + note[2:3]
        gain_ref[g] = jnp.broadcast_to(gain, (8, LANES))
    mixed = residual_ref[...].astype(F32) + jnp.concatenate(halves, axis=0)
    mixed_ref[...] = mixed
    out_ref[...] = dot(place_ref[...], mixed.astype(BF16)).astype(BF16)


def spread_body(in_ref, drop_ref, out_ref):
    span = BLOCKS * CAP_PAD
    for r in range(GROUPS):
        kept = dot(drop_ref[...], in_ref[r * span : (r + 1) * span, :]).astype(BF16)
        for g in range(r, N_TP, GROUPS):
            out_ref[g] = kept


def expert_body(in_ref, gain_ref, *refs):
    many = 3 * GROUPS
    far, (out_ref, x_ref), weights, sems = refs[:many], refs[many : many + 2], refs[many + 2 : -1], refs[-1]
    copies = [pltpu.make_async_copy(far[i], weights[i], sems.at[i]) for i in range(many)]
    for copy in copies:
        copy.start()
    total = jnp.zeros((ROWS, LANES), F32)
    for g in range(N_TP):
        x = in_ref[g].astype(F32)
        total = total + x * x
    scale = lax.rsqrt(jnp.sum(total, axis=1, keepdims=True) * (1.0 / D) + EPSILON)
    for g in range(N_TP):
        x = in_ref[g].astype(F32) * scale * gain_ref[g, 0:1, :]
        x_ref[:, g * LANES : (g + 1) * LANES] = x.astype(BF16)
    hidden = []
    for i in range(GROUPS):
        copies[2 * i].wait()
        gate = jnp.minimum(dot(x_ref[...], weights[2 * i][...]), CLAMP_LIMIT)
        copies[2 * i + 1].wait()
        up = jnp.clip(dot(x_ref[...], weights[2 * i + 1][...]), -CLAMP_LIMIT, CLAMP_LIMIT)
        unit = gate * (1.0 / (1.0 + jnp.exp(-SIGMOID_SCALE * gate))) * (up + 1.0)
        hidden.append(unit.astype(BF16))
    for copy in copies[2 * GROUPS :]:
        copy.wait()
    downs = weights[2 * GROUPS :]
    for g in range(0, N_TP, 2):
        cols = slice(g * LANES, (g + 2) * LANES)
        part = dot(hidden[0], downs[0][:, cols])
        for h, w in zip(hidden[1:], downs[1:]):
            part = part + dot(h, w[:, cols])
        part = part.astype(BF16)
        out_ref[g] = part[:, :LANES]
        out_ref[g + 1] = part[:, LANES:]


def gather_body(in_ref, widen_ref, out_ref):
    span = BLOCKS * CAP_PAD
    for r in range(GROUPS):
        total = in_ref[r].astype(F32)
        for g in range(r + GROUPS, N_TP, GROUPS):
            total = total + in_ref[g].astype(F32)
        rows = dot(widen_ref[...], total.astype(BF16)).astype(BF16)
        out_ref[r * span : (r + 1) * span, :] = rows


def finish_body(in_ref, mix0_ref, mix1_ref, mix2_ref, mixed_ref, out_ref):
    total = mixed_ref[...]
    rows = in_ref[...]
    for mix_ref in (mix0_ref, mix1_ref, mix2_ref):
        total = total + dot(mix_ref[...], rows)
    out_ref[...] = total.astype(BF16)


def shaped(shape, dtype=BF16):
    return pltpu.VMEM(shape, dtype)


VMEM = pl.BlockSpec(memory_space=pltpu.VMEM)
SMEM = pl.BlockSpec(memory_space=pltpu.SMEM)
HBM = pl.BlockSpec(memory_space=pltpu.HBM)


def call(body, outs, *args, scratch=(), mib=8, far=0):
    near = len(args) - far
    specs = [SMEM if a.shape == (1,) else VMEM for a in args[:near]] + [HBM] * far
    args = args[:near] + tuple(pltpu.with_memory_space_constraint(a, pltpu.HBM) for a in args[near:])
    many = isinstance(outs, (list, tuple))
    return pl.pallas_call(
        body,
        out_shape=outs,
        in_specs=specs,
        out_specs=[VMEM] * len(outs) if many else VMEM,
        scratch_shapes=list(scratch),
        compiler_params=pltpu.CompilerParams(vmem_limit_bytes=mib * 1024 * 1024),
    )(*args)


def exchange(x, axes):
    return lax.all_to_all(x, axes, 0, 0, tiled=True)


def shifted(x, axis, size, by):
    return lax.ppermute(x, axis, [(i, (i + by) % size) for i in range(size)])


def partner(x):
    return lax.ppermute(x, "c", [(0, 1), (1, 0)])


def neighbour(x):
    return lax.ppermute(x, "y", [(i, i ^ 1) for i in range(N_Y)])


def per_device(
    queries,
    keys,
    values,
    docs,
    query_gain,
    key_gain,
    out_weight,
    residual,
    norm_gain,
    routes,
    route_weight,
    gate_weight,
    up_weight,
    down_weight,
):
    return step(
        queries,
        keys.T,
        values.T,
        docs.reshape(2, LANES),
        query_gain.reshape(1, HD),
        key_gain.reshape(1, HD),
        out_weight,
        residual,
        norm_gain,
        routes.T,
        route_weight.T,
        gate_weight[0],
        up_weight[0],
        down_weight[0],
    )


def step(
    queries,
    keys,
    values,
    docs,
    query_gain,
    key_gain,
    out_weight,
    residual,
    norm_gain,
    routes,
    route_weight,
    gate,
    up,
    down,
):
    row_tab, col_tab = tables()
    drop = compaction()
    block = (lax.axis_index("z") * N_X + lax.axis_index("x")).reshape(1).astype(jnp.int32)
    spot = lax.axis_index("x").reshape(1).astype(jnp.int32)
    core = lax.axis_index("c").reshape(1).astype(jnp.int32)
    sources = (
        queries,
        keys,
        values,
        docs,
        query_gain,
        key_gain,
        jnp.asarray(row_tab),
        jnp.asarray(col_tab),
    )
    kept = [pltpu.VMEM(a.shape[1:] if i == 6 else a.shape, a.dtype) for i, a in enumerate(sources)]
    qs, kvs = call(
        prep_body,
        [shaped((TOK + NOTE, LANES)), shaped((N_Z, TOK + NOTE, LANES))],
        block,
        *sources,
        scratch=kept + [pltpu.SemaphoreType.DMA((len(sources),))],
        far=len(sources),
    )
    kv_all = exchange(kvs, "z")
    q_all = [qs] + [shifted(qs, "x", N_X, i) for i in range(1, N_X)]
    out_other = partner(out_weight)
    gate_y, up_y = neighbour(gate), neighbour(up)
    down_y = neighbour(down)
    gate_o, up_o = partner(gate), partner(up)
    down_o = partner(down)
    gate_yo, up_yo = partner(gate_y), partner(up_y)
    down_yo = partner(down_y)
    slot_table = shaped((EXPERTS * CAP_PAD, TOK))
    mix_table = shaped((TOK, EXPERTS * CAP_PAD))
    place = call(route_body, slot_table, routes)
    mixes = [
        call(functools.partial(mix_body, i), mix_table, routes, route_weight)
        for i in range(3)
    ]
    partial = call(
        attend_body,
        shaped((N_X * 2, HALF + NOTE, LANES)),
        spot,
        *q_all,
        kv_all,
        scratch=[
            pltpu.VMEM((N_X, TOK + NOTE, LANES), BF16),
            pltpu.VMEM((N_Z * TOK, LANES), BF16),
            pltpu.VMEM((N_Z * TOK, LANES), BF16),
        ],
        mib=24,
    )
    partial = exchange(partial, ("x", "c"))
    projected = call(
        project_body,
        shaped((N_TP, HALF + NOTE, LANES)),
        core,
        partial,
        out_weight,
        out_other,
        norm_gain.reshape(1, LANES),
    )
    projected = exchange(projected, ("y", "c"))
    mixed, gain_all, outgoing = call(
        dispatch_body,
        [
            shaped((TOK, LANES), F32),
            shaped((N_TP, 8, LANES), F32),
            shaped((EXPERTS * CAP_PAD, LANES)),
        ],
        projected,
        residual,
        place,
    )
    arrived = exchange(outgoing.reshape(N_SP, CAP_PAD, LANES), ("z", "x"))
    spread = call(
        spread_body,
        shaped((N_TP, ROWS, LANES)),
        arrived.reshape(N_SP * CAP_PAD, LANES),
        jnp.asarray(drop, BF16),
    )
    columns = exchange(spread, ("y", "c"))
    weights = (gate, up, gate_o, up_o, gate_y, up_y, gate_yo, up_yo, down, down_o, down_y, down_yo)
    parts = call(
        expert_body,
        shaped((N_TP, ROWS, LANES)),
        columns,
        gain_all,
        *weights,
        scratch=[pltpu.VMEM((ROWS, D), BF16)]
        + [pltpu.VMEM(w.shape, BF16) for w in weights]
        + [pltpu.SemaphoreType.DMA((len(weights),))],
        mib=32,
        far=len(weights),
    )
    parts = exchange(parts, ("y", "c"))
    expert_out = call(
        gather_body, shaped((N_SP * CAP_PAD, LANES)), parts, jnp.asarray(drop.T, BF16)
    )
    returned = exchange(expert_out.reshape(N_SP, CAP_PAD, LANES), ("z", "x"))
    return call(
        finish_body,
        jax.ShapeDtypeStruct((TOK, LANES), BF16),
        returned.reshape(N_SP * CAP_PAD, LANES),
        *mixes,
        mixed,
    )


def solution(mesh):
    grid = Mesh(mesh.devices.reshape(N_Z, N_X, N_Y, N_C), ("z", "x", "y", "c"))
    sp, tp = ("z", "x"), ("y", "c")
    in_specs = (
        P(sp, tp),
        P(sp, tp),
        P(sp, tp),
        P(sp),
        P(),
        P(),
        P(tp, None),
        P(sp, tp),
        P(tp),
        P(sp, None),
        P(sp, None),
        P(sp, None, tp),
        P(sp, None, tp),
        P(sp, tp, None),
    )
    return jax.shard_map(
        per_device, mesh=grid, in_specs=in_specs, out_specs=P(sp, tp), check_vma=False
    )
```

```python
import functools

import jax
import jax.numpy as jnp
import numpy as np
from jax import lax
from jax.experimental import pallas as pl
from jax.experimental.pallas import tpu as pltpu
from jax.sharding import Mesh, PartitionSpec as P


GRID_W = 64
EPSILON = 1e-06
ROTARY_BASE = 10000.0
CLAMP_LIMIT = 7.0
SIGMOID_SCALE = 1.702
N_Z, N_X, N_Y, N_C = 8, 4, 8, 2
N_SP, N_TP = N_Z * N_X, N_Y * N_C
TOK = 256
HALF = TOK // 2
HD = 64
LANES = 128
D = 2048
EXPERTS = 32
CAP = 20
CAP_PAD = 24
GROUPS = 4
ROWS = N_SP * CAP // GROUPS
BLOCKS = N_SP // GROUPS
NOTE = 16
MASK_BIG = 16384.0
WINDOWS = (5, 6, N_Z)

F32 = jnp.float32
BF16 = jnp.bfloat16


def tables():
    quarter = HD // 4
    freqs = (ROTARY_BASE ** (-np.arange(quarter, dtype=np.float32) / quarter)).astype(np.float32)
    lane = np.arange(LANES)
    pair = (lane % HD) // 2
    is_row = pair < quarter
    freq = freqs[np.where(is_row, pair, pair - quarter)]
    sign = np.where(lane % 2 == 0, -1.0, 1.0)
    cols = (np.arange(GRID_W, dtype=np.float32)[:, None] * freq).astype(np.float32)
    rows = (np.arange(N_SP * TOK // GRID_W, dtype=np.float32)[:, None] * freq).astype(np.float32)
    cols, rows = cols.astype(np.float64), rows.astype(np.float64)
    keep = lambda a, m: np.where(m, a, 0.0).astype(np.float32)
    per = TOK // GRID_W
    row_c = keep(np.cos(rows), is_row).reshape(N_SP, per, LANES)
    row_s = keep(np.sin(rows) * sign, is_row).reshape(N_SP, per, LANES)
    row_tab = np.concatenate([row_c, row_s], axis=1)
    col_tab = np.stack([keep(np.cos(cols), ~is_row), keep(np.sin(cols) * sign, ~is_row)])
    return row_tab, col_tab


def compaction():
    out = np.zeros((ROWS, BLOCKS * CAP_PAD), np.float32)
    r = np.arange(ROWS)
    out[r, (r // CAP) * CAP_PAD + r % CAP] = 1.0
    return out


def dot(a, b, ca=1, cb=0):
    return lax.dot_general(a, b, (((ca,), (cb,)), ((), ())), preferred_element_type=F32)


def iota(shape, dim):
    return lax.broadcasted_iota(jnp.int32, shape, dim)


def prep_body(blk, *refs):
    sources, (qs_ref, kvs_ref), kept, sems = refs[:8], refs[8:10], refs[10:18], refs[18]
    copies = []
    for i, (src, dst) in enumerate(zip(sources, kept)):
        src = src.at[blk[0]] if i == 6 else src
        copies.append(pltpu.make_async_copy(src, dst, sems.at[i]))
    for copy in copies:
        copy.start()
    for copy in copies:
        copy.wait()
    q_ref, k_ref, v_ref, docs_ref, qg_ref, kg_ref, row_ref, col_ref = kept
    lane = iota((TOK, LANES), 1)
    low = lane < HD
    even = (lane & 1) == 0
    rows = row_ref[...]
    per = TOK // GRID_W
    cos_t = jnp.concatenate([col_ref[0] + rows[j : j + 1] for j in range(per)], axis=0)
    sin_t = jnp.concatenate([col_ref[1] + rows[per + j : per + j + 1] for j in range(per)], axis=0)

    def turn(n):
        swapped = jnp.where(even, pltpu.roll(n, LANES - 1, 1), pltpu.roll(n, 1, 1))
        return n * cos_t + swapped * sin_t

    x = q_ref[...].astype(F32)
    sq = x * x
    s0 = jnp.sum(jnp.where(low, sq, 0.0), axis=1, keepdims=True)
    s1 = jnp.sum(jnp.where(low, 0.0, sq), axis=1, keepdims=True)
    r0 = lax.rsqrt(s0 * (1.0 / HD) + EPSILON)
    r1 = lax.rsqrt(s1 * (1.0 / HD) + EPSILON)
    gain = jnp.concatenate([qg_ref[...], qg_ref[...]], axis=1)
    q_out = turn(x * jnp.where(low, r0, r1) * gain).astype(BF16)

    kv = jnp.concatenate([k_ref[...], v_ref[...]], axis=0).astype(F32).T
    sk = jnp.sum(jnp.where(low, kv * kv, 0.0), axis=1, keepdims=True)
    rk = lax.rsqrt(sk * (1.0 / HD) + EPSILON)
    gain_k = jnp.concatenate([kg_ref[...], kg_ref[...]], axis=1)
    kv_out = jnp.where(low, turn(kv * rk * gain_k), kv).astype(BF16)

    docs = docs_ref[...]
    n0 = jnp.sum((docs < 1).astype(F32))
    n1 = jnp.sum((docs < 2).astype(F32))
    row = iota((NOTE, LANES), 0)
    note = jnp.where(row == 0, n0, jnp.where(row == 1, n1, 0.0)).astype(BF16)
    qs_ref[:TOK, :] = q_out
    qs_ref[TOK:, :] = note
    for i in range(N_Z):
        kvs_ref[i, :TOK, :] = kv_out
        kvs_ref[i, TOK:, :] = note


def split3(x):
    hi = x.astype(BF16).astype(F32)
    mid = (x - hi).astype(BF16).astype(F32)
    return hi, mid, x - hi - mid


def attend_body(spot, *refs):
    q_refs, (kv_ref, out_ref, q_ref, kp_ref, vp_ref, plan_ref) = refs[:N_X], refs[N_X:]
    for i in range(N_X):
        q_ref[i] = q_refs[i][...]
    lane = iota((TOK, LANES), 1)
    low = lane < HD
    idx = iota((TOK, LANES), 0).astype(F32)

    def doc_of(note):
        n0 = note[0:1, :].astype(F32)
        n1 = note[1:2, :].astype(F32)
        return jnp.where(idx < n0, HD, jnp.where(idx < n1, HD + 1, HD + 2))

    for j in range(N_Z):
        kv = kv_ref[j, :TOK, :]
        mark = (doc_of(kv_ref[j, TOK:, :]) == lane).astype(F32)
        kvf = kv.astype(F32)
        kp_ref[j * TOK : (j + 1) * TOK, :] = jnp.where(low, kvf, mark).astype(BF16)
        vp_ref[j * TOK : (j + 1) * TOK, :] = jnp.where(low, 1.0, kvf).astype(BF16)

    def documents(note):
        n0, n1 = note[0:1, :].astype(F32), note[1:2, :].astype(F32)
        one = jnp.ones((1, LANES), F32)
        least = jnp.where(n0 <= 0.0, one, 0.0) + jnp.where(n1 <= 0.0, one, 0.0)
        most = jnp.where(n0 < TOK, one, 0.0) + jnp.where(n1 < TOK, one, 0.0)
        return least, most

    ranges = [documents(kv_ref[j, TOK:, :]) for j in range(N_Z)]
    for b in range(N_X):
        least, most = documents(q_ref[b, TOK:, :])
        first = jnp.full((1, LANES), float(N_Z), F32)
        last = jnp.full((1, LANES), -1.0, F32)
        for j, (low_doc, high_doc) in enumerate(ranges):
            meet = (low_doc <= most) & (least <= high_doc)
            first = jnp.where(meet, jnp.minimum(first, float(j)), first)
            last = jnp.where(meet, float(j), last)
        code = jnp.where(last < 0.0, 0.0, first * 16.0 + (last - first + 1.0))
        plan_ref[b] = jnp.max(code).astype(jnp.int32)
    eye = (iota((HALF, LANES), 0) == iota((HALF, LANES), 1)).astype(BF16)
    lane_h = iota((HALF, LANES), 1)

    def block(b, start, size):
        qf = q_ref[b, :TOK, :].astype(F32) * (HD**-0.5)
        doc = doc_of(q_ref[b, TOK:, :])
        other = jnp.where((doc == lane) | (lane > HD + 2), 0.0, -MASK_BIG)
        keys = pl.ds(start * TOK, size * TOK)
        heads = []
        for h in range(2):
            qh = qf if h == 0 else pltpu.roll(qf, HD, 1)
            qp = jnp.where(low, qh, other).astype(BF16)
            s = dot(qp, kp_ref[keys, :], 1, 1)
            peak = jnp.max(s, axis=1, keepdims=True)
            p = jnp.exp(s - peak).astype(BF16)
            acc = dot(p, vp_ref[keys, :])
            total = acc[:, 0:1]
            o = acc / total
            heads.append((pltpu.roll(o, HD, 1) if h == 0 else o, peak + jnp.log(total)))
        o = jnp.where(low, heads[0][0], heads[1][0]).astype(BF16)
        parts = split3(heads[0][1]) + split3(heads[1][1])
        for half in range(2):
            rows = slice(half * HALF, (half + 1) * HALF)
            stat = jnp.zeros((HALF, LANES), F32)
            for i, part in enumerate(parts):
                stat = jnp.where(lane_h == i, part[rows], stat)
            stat_t = dot(stat.astype(BF16), eye, 0, 0)
            to = lax.rem(spot[0] + N_X - b, N_X) * 2 + half
            out_ref[to, :HALF, :] = o[rows]
            out_ref[to, HALF:, :] = stat_t[:NOTE].astype(BF16)

    def step(b, carry):
        code = plan_ref[b]
        first, count = code // 16, code % 16
        fewer = -1
        for size in WINDOWS:

            @pl.when((count > fewer) & (count <= size))
            def _(size=size):
                start = 0 if size == N_Z else jnp.minimum(first, N_Z - size)
                block(b, start, size)

            fewer = size
        return carry

    lax.fori_loop(0, N_X, step, 0)


def project_body(core, in_ref, w_own_ref, w_other_ref, gain_ref, out_ref):
    gain = split3(gain_ref[...])
    row = iota((NOTE, LANES), 0)
    lane = iota((NOTE, LANES), 1)
    pick = (((row < 3) & (lane < HD)) | ((row >= 3) & (row < 6) & (lane >= HD))).astype(BF16)

    def attended(c):
        lse = [dot(in_ref[x * 2 + c, HALF:, :], pick, 0, 0) for x in range(N_X)]
        top = functools.reduce(jnp.maximum, lse)
        total = jnp.zeros((HALF, LANES), F32)
        mixed = jnp.zeros((HALF, LANES), F32)
        for x in range(N_X):
            w = jnp.exp(lse[x] - top)
            total = total + w
            mixed = mixed + w * in_ref[x * 2 + c, :HALF, :].astype(F32)
        return (mixed / total).astype(BF16)

    note = jnp.where(row == 0, gain[0], jnp.where(row == 1, gain[1], jnp.where(row == 2, gain[2], 0.0)))
    own = attended(core[0])
    other = attended(1 - core[0])
    for g in range(N_TP):
        cols = slice(g * LANES, (g + 1) * LANES)
        part = dot(own, w_own_ref[:, cols]) + dot(other, w_other_ref[:, cols])
        out_ref[g, :HALF, :] = part.astype(BF16)
        out_ref[g, HALF:, :] = note.astype(BF16)


def slots_of(routes_ref):
    expert = iota((EXPERTS, TOK), 0)
    r0, r1 = routes_ref[0:1, :], routes_ref[1:2, :]
    named = ((expert == r0) | (expert == r1)).astype(F32)
    before = (iota((TOK, TOK), 0) < iota((TOK, TOK), 1)).astype(BF16)
    slot = dot(named.astype(BF16), before)
    return expert == r0, expert == r1, jnp.where(named > 0.0, slot, -1.0)


def laid_out(slot, value, write):
    slots = iota((CAP_PAD, TOK), 0).astype(F32)
    for e in range(0, EXPERTS, 2):
        both = [jnp.where(slots == slot[i : i + 1, :], value(i), 0.0) for i in (e, e + 1)]
        write(slice(e * CAP_PAD, (e + 2) * CAP_PAD), jnp.concatenate(both, axis=0).astype(BF16))


def route_body(routes_ref, place_ref):
    _, _, slot = slots_of(routes_ref)

    def write(rows, value):
        place_ref[rows, :] = value

    laid_out(slot, lambda e: 1.0, write)


def mix_body(term, routes_ref, weight_ref, mix_ref):
    first, second, slot = slots_of(routes_ref)
    weight = jnp.where(first, weight_ref[0:1, :], jnp.where(second, weight_ref[1:2, :], 0.0))
    part = split3(weight)[term]

    parts = []
    laid_out(slot, lambda e: part[e : e + 1, :], lambda rows, value: parts.append(value))
    for i in range(0, len(parts), 8):
        some = jnp.concatenate(parts[i : i + 8], axis=0).astype(F32)
        mix_ref[:, i * 2 * CAP_PAD : (i + 8) * 2 * CAP_PAD] = some.T.astype(BF16)


def dispatch_body(in_ref, residual_ref, place_ref, mixed_ref, gain_ref, out_ref):
    halves = []
    for c in range(2):
        total = in_ref[c, :HALF, :].astype(F32)
        for y in range(1, N_Y):
            total = total + in_ref[y * 2 + c, :HALF, :].astype(F32)
        halves.append(total)
    for g in range(N_TP):
        note = in_ref[g, HALF:, :].astype(F32)
        gain = note[0:1] + note[1:2] + note[2:3]
        gain_ref[g] = jnp.broadcast_to(gain, (8, LANES))
    mixed = residual_ref[...].astype(F32) + jnp.concatenate(halves, axis=0)
    mixed_ref[...] = mixed
    out_ref[...] = dot(place_ref[...], mixed.astype(BF16)).astype(BF16)


def spread_body(in_ref, drop_ref, out_ref):
    span = BLOCKS * CAP_PAD
    for r in range(GROUPS):
        kept = dot(drop_ref[...], in_ref[r * span : (r + 1) * span, :]).astype(BF16)
        for g in range(r, N_TP, GROUPS):
            out_ref[g] = kept


def expert_body(in_ref, gain_ref, late_ref, *refs):
    many = 3 * GROUPS - 1
    far, (out_ref, x_ref), weights, sems = refs[:many], refs[many : many + 2], refs[many + 2 : -1], refs[-1]
    copies = [pltpu.make_async_copy(far[i], weights[i], sems.at[i]) for i in range(many)]
    for copy in copies:
        copy.start()
    total = jnp.zeros((ROWS, LANES), F32)
    for g in range(N_TP):
        x = in_ref[g].astype(F32)
        total = total + x * x
    scale = lax.rsqrt(jnp.sum(total, axis=1, keepdims=True) * (1.0 / D) + EPSILON)
    for g in range(N_TP):
        x = in_ref[g].astype(F32) * scale * gain_ref[g, 0:1, :]
        x_ref[:, g * LANES : (g + 1) * LANES] = x.astype(BF16)
    hidden = []
    for i in range(GROUPS):
        copies[2 * i].wait()
        gate = jnp.minimum(dot(x_ref[...], weights[2 * i][...]), CLAMP_LIMIT)
        copies[2 * i + 1].wait()
        up = jnp.clip(dot(x_ref[...], weights[2 * i + 1][...]), -CLAMP_LIMIT, CLAMP_LIMIT)
        unit = gate * (1.0 / (1.0 + jnp.exp(-SIGMOID_SCALE * gate))) * (up + 1.0)
        hidden.append(unit.astype(BF16))
    for copy in copies[2 * GROUPS :]:
        copy.wait()
    downs = weights[2 * GROUPS :] + (late_ref,)
    for g in range(0, N_TP, 2):
        cols = slice(g * LANES, (g + 2) * LANES)
        part = dot(hidden[0], downs[0][:, cols])
        for h, w in zip(hidden[1:], downs[1:]):
            part = part + dot(h, w[:, cols])
        part = part.astype(BF16)
        out_ref[g] = part[:, :LANES]
        out_ref[g + 1] = part[:, LANES:]


def gather_body(in_ref, widen_ref, out_ref):
    span = BLOCKS * CAP_PAD
    for r in range(GROUPS):
        total = in_ref[r].astype(F32)
        for g in range(r + GROUPS, N_TP, GROUPS):
            total = total + in_ref[g].astype(F32)
        rows = dot(widen_ref[...], total.astype(BF16)).astype(BF16)
        out_ref[r * span : (r + 1) * span, :] = rows


def finish_body(in_ref, mix0_ref, mix1_ref, mix2_ref, mixed_ref, out_ref):
    total = mixed_ref[...]
    rows = in_ref[...]
    for mix_ref in (mix0_ref, mix1_ref, mix2_ref):
        total = total + dot(mix_ref[...], rows)
    out_ref[...] = total.astype(BF16)


def shaped(shape, dtype=BF16):
    return pltpu.VMEM(shape, dtype)


VMEM = pl.BlockSpec(memory_space=pltpu.VMEM)
SMEM = pl.BlockSpec(memory_space=pltpu.SMEM)
HBM = pl.BlockSpec(memory_space=pltpu.HBM)


def call(body, outs, *args, scratch=(), mib=8, far=0):
    near = len(args) - far
    specs = [SMEM if a.shape == (1,) else VMEM for a in args[:near]] + [HBM] * far
    args = args[:near] + tuple(pltpu.with_memory_space_constraint(a, pltpu.HBM) for a in args[near:])
    many = isinstance(outs, (list, tuple))
    return pl.pallas_call(
        body,
        out_shape=outs,
        in_specs=specs,
        out_specs=[VMEM] * len(outs) if many else VMEM,
        scratch_shapes=list(scratch),
        compiler_params=pltpu.CompilerParams(vmem_limit_bytes=mib * 1024 * 1024),
    )(*args)


def exchange(x, axes):
    return lax.all_to_all(x, axes, 0, 0, tiled=True)


def shifted(x, axis, size, by):
    return lax.ppermute(x, axis, [(i, (i + by) % size) for i in range(size)])


def partner(x):
    return lax.ppermute(x, "c", [(0, 1), (1, 0)])


def neighbour(x):
    return lax.ppermute(x, "y", [(i, i ^ 1) for i in range(N_Y)])


def per_device(
    queries,
    keys,
    values,
    docs,
    query_gain,
    key_gain,
    out_weight,
    residual,
    norm_gain,
    routes,
    route_weight,
    gate_weight,
    up_weight,
    down_weight,
):
    return step(
        queries,
        keys.T,
        values.T,
        docs.reshape(2, LANES),
        query_gain.reshape(1, HD),
        key_gain.reshape(1, HD),
        out_weight,
        residual,
        norm_gain,
        routes.T,
        route_weight.T,
        gate_weight[0],
        up_weight[0],
        down_weight[0],
    )


def step(
    queries,
    keys,
    values,
    docs,
    query_gain,
    key_gain,
    out_weight,
    residual,
    norm_gain,
    routes,
    route_weight,
    gate,
    up,
    down,
):
    row_tab, col_tab = tables()
    drop = compaction()
    block = (lax.axis_index("z") * N_X + lax.axis_index("x")).reshape(1).astype(jnp.int32)
    spot = lax.axis_index("x").reshape(1).astype(jnp.int32)
    core = lax.axis_index("c").reshape(1).astype(jnp.int32)
    sources = (
        queries,
        keys,
        values,
        docs,
        query_gain,
        key_gain,
        jnp.asarray(row_tab),
        jnp.asarray(col_tab),
    )
    kept = [pltpu.VMEM(a.shape[1:] if i == 6 else a.shape, a.dtype) for i, a in enumerate(sources)]
    qs, kvs = call(
        prep_body,
        [shaped((TOK + NOTE, LANES)), shaped((N_Z, TOK + NOTE, LANES))],
        block,
        *sources,
        scratch=kept + [pltpu.SemaphoreType.DMA((len(sources),))],
        far=len(sources),
    )
    kv_all = exchange(kvs, "z")
    q_all = [qs] + [shifted(qs, "x", N_X, i) for i in range(1, N_X)]
    out_other = partner(out_weight)
    gate_y, up_y = neighbour(gate), neighbour(up)
    down_y = neighbour(down)
    gate_o, up_o = partner(gate), partner(up)
    down_o = partner(down)
    gate_yo, up_yo = partner(gate_y), partner(up_y)
    down_yo = partner(down_y)
    slot_table = shaped((EXPERTS * CAP_PAD, TOK))
    mix_table = shaped((TOK, EXPERTS * CAP_PAD))
    place = call(route_body, slot_table, routes)
    mixes = [
        call(functools.partial(mix_body, i), mix_table, routes, route_weight)
        for i in range(3)
    ]
    partial = call(
        attend_body,
        shaped((N_X * 2, HALF + NOTE, LANES)),
        spot,
        *q_all,
        kv_all,
        scratch=[
            pltpu.VMEM((N_X, TOK + NOTE, LANES), BF16),
            pltpu.VMEM((N_Z * TOK, LANES), BF16),
            pltpu.VMEM((N_Z * TOK, LANES), BF16),
            pltpu.SMEM((N_X,), jnp.int32),
        ],
        mib=24,
    )
    partial = exchange(partial, ("x", "c"))
    projected = call(
        project_body,
        shaped((N_TP, HALF + NOTE, LANES)),
        core,
        partial,
        out_weight,
        out_other,
        norm_gain.reshape(1, LANES),
    )
    projected = exchange(projected, ("y", "c"))
    mixed, gain_all, outgoing = call(
        dispatch_body,
        [
            shaped((TOK, LANES), F32),
            shaped((N_TP, 8, LANES), F32),
            shaped((EXPERTS * CAP_PAD, LANES)),
        ],
        projected,
        residual,
        place,
    )
    arrived = exchange(outgoing.reshape(N_SP, CAP_PAD, LANES), ("z", "x"))
    spread = call(
        spread_body,
        shaped((N_TP, ROWS, LANES)),
        arrived.reshape(N_SP * CAP_PAD, LANES),
        jnp.asarray(drop, BF16),
    )
    columns = exchange(spread, ("y", "c"))
    weights = (gate, up, gate_o, up_o, gate_y, up_y, gate_yo, up_yo, down, down_o, down_y)
    parts = call(
        expert_body,
        shaped((N_TP, ROWS, LANES)),
        columns,
        gain_all,
        down_yo,
        *weights,
        scratch=[pltpu.VMEM((ROWS, D), BF16)]
        + [pltpu.VMEM(w.shape, BF16) for w in weights]
        + [pltpu.SemaphoreType.DMA((len(weights),))],
        mib=32,
        far=len(weights),
    )
    parts = exchange(parts, ("y", "c"))
    expert_out = call(
        gather_body, shaped((N_SP * CAP_PAD, LANES)), parts, jnp.asarray(drop.T, BF16)
    )
    returned = exchange(expert_out.reshape(N_SP, CAP_PAD, LANES), ("z", "x"))
    return call(
        finish_body,
        jax.ShapeDtypeStruct((TOK, LANES), BF16),
        returned.reshape(N_SP * CAP_PAD, LANES),
        *mixes,
        mixed,
    )


def solution(mesh):
    grid = Mesh(mesh.devices.reshape(N_Z, N_X, N_Y, N_C), ("z", "x", "y", "c"))
    sp, tp = ("z", "x"), ("y", "c")
    in_specs = (
        P(sp, tp),
        P(sp, tp),
        P(sp, tp),
        P(sp),
        P(),
        P(),
        P(tp, None),
        P(sp, tp),
        P(tp),
        P(sp, None),
        P(sp, None),
        P(sp, None, tp),
        P(sp, None, tp),
        P(sp, tp, None),
    )
    return jax.shard_map(
        per_device, mesh=grid, in_specs=in_specs, out_specs=P(sp, tp), check_vma=False
    )
```

```python
import functools

import jax
import jax.numpy as jnp
import numpy as np
from jax import lax
from jax.experimental import pallas as pl
from jax.experimental.pallas import tpu as pltpu
from jax.sharding import Mesh, PartitionSpec as P


GRID_W = 64
EPSILON = 1e-06
ROTARY_BASE = 10000.0
CLAMP_LIMIT = 7.0
SIGMOID_SCALE = 1.702
N_Z, N_X, N_Y, N_C = 8, 4, 8, 2
N_SP, N_TP = N_Z * N_X, N_Y * N_C
TOK = 256
HALF = TOK // 2
HD = 64
LANES = 128
D = 2048
EXPERTS = 32
CAP = 20
CAP_PAD = 24
GROUPS = 4
ROWS = N_SP * CAP // GROUPS
BLOCKS = N_SP // GROUPS
NOTE = 16
MASK_BIG = 16384.0
WINDOWS = (5, 6, N_Z)

F32 = jnp.float32
BF16 = jnp.bfloat16


def tables():
    quarter = HD // 4
    freqs = (ROTARY_BASE ** (-np.arange(quarter, dtype=np.float32) / quarter)).astype(np.float32)
    lane = np.arange(LANES)
    pair = (lane % HD) // 2
    is_row = pair < quarter
    freq = freqs[np.where(is_row, pair, pair - quarter)]
    sign = np.where(lane % 2 == 0, -1.0, 1.0)
    cols = (np.arange(GRID_W, dtype=np.float32)[:, None] * freq).astype(np.float32)
    rows = (np.arange(N_SP * TOK // GRID_W, dtype=np.float32)[:, None] * freq).astype(np.float32)
    cols, rows = cols.astype(np.float64), rows.astype(np.float64)
    keep = lambda a, m: np.where(m, a, 0.0).astype(np.float32)
    per = TOK // GRID_W
    row_c = keep(np.cos(rows), is_row).reshape(N_SP, per, LANES)
    row_s = keep(np.sin(rows) * sign, is_row).reshape(N_SP, per, LANES)
    row_tab = np.concatenate([row_c, row_s], axis=1)
    col_tab = np.stack([keep(np.cos(cols), ~is_row), keep(np.sin(cols) * sign, ~is_row)])
    return row_tab, col_tab


def compaction():
    out = np.zeros((ROWS, BLOCKS * CAP_PAD), np.float32)
    r = np.arange(ROWS)
    out[r, (r // CAP) * CAP_PAD + r % CAP] = 1.0
    return out


def dot(a, b, ca=1, cb=0):
    return lax.dot_general(a, b, (((ca,), (cb,)), ((), ())), preferred_element_type=F32)


def iota(shape, dim):
    return lax.broadcasted_iota(jnp.int32, shape, dim)


def prep_body(blk, *refs):
    sources, (qs_ref, kvs_ref), kept, sems = refs[:8], refs[8:10], refs[10:18], refs[18]
    copies = []
    for i, (src, dst) in enumerate(zip(sources, kept)):
        src = src.at[blk[0]] if i == 6 else src
        copies.append(pltpu.make_async_copy(src, dst, sems.at[i]))
    for copy in copies:
        copy.start()
    for copy in copies:
        copy.wait()
    q_ref, k_ref, v_ref, docs_ref, qg_ref, kg_ref, row_ref, col_ref = kept
    lane = iota((TOK, LANES), 1)
    low = lane < HD
    even = (lane & 1) == 0
    rows = row_ref[...]
    per = TOK // GRID_W
    cos_t = jnp.concatenate([col_ref[0] + rows[j : j + 1] for j in range(per)], axis=0)
    sin_t = jnp.concatenate([col_ref[1] + rows[per + j : per + j + 1] for j in range(per)], axis=0)

    def turn(n):
        swapped = jnp.where(even, pltpu.roll(n, LANES - 1, 1), pltpu.roll(n, 1, 1))
        return n * cos_t + swapped * sin_t

    x = q_ref[...].astype(F32)
    sq = x * x
    s0 = jnp.sum(jnp.where(low, sq, 0.0), axis=1, keepdims=True)
    s1 = jnp.sum(jnp.where(low, 0.0, sq), axis=1, keepdims=True)
    r0 = lax.rsqrt(s0 * (1.0 / HD) + EPSILON)
    r1 = lax.rsqrt(s1 * (1.0 / HD) + EPSILON)
    gain = jnp.concatenate([qg_ref[...], qg_ref[...]], axis=1)
    q_out = turn(x * jnp.where(low, r0, r1) * gain).astype(BF16)

    flat = k_ref[...].astype(F32)
    k = jnp.concatenate([flat, jnp.zeros_like(flat)], axis=0).T
    rk = lax.rsqrt(jnp.sum(k * k, axis=1, keepdims=True) * (1.0 / HD) + EPSILON)
    gain_k = jnp.concatenate([kg_ref[...], kg_ref[...]], axis=1)
    k = turn(k * rk * gain_k)
    keys = jnp.where(low[:HALF], k[:HALF], pltpu.roll(k[HALF:], HD, 1)).astype(BF16)
    values = v_ref[...]

    docs = docs_ref[...]
    n0 = jnp.sum((docs < 1).astype(F32))
    n1 = jnp.sum((docs < 2).astype(F32))
    row = iota((NOTE, LANES), 0)
    note = jnp.where(row == 0, n0, jnp.where(row == 1, n1, 0.0)).astype(BF16)
    qs_ref[:TOK, :] = q_out
    qs_ref[TOK:, :] = note
    for i in range(N_Z):
        kvs_ref[i, :HALF, :] = keys
        kvs_ref[i, HALF : HALF + HD, :] = values[:, :HALF]
        kvs_ref[i, HALF + HD : TOK, :] = values[:, HALF:]
        kvs_ref[i, TOK:, :] = note


def split3(x):
    hi = x.astype(BF16).astype(F32)
    mid = (x - hi).astype(BF16).astype(F32)
    return hi, mid, x - hi - mid


def attend_body(spot, *refs):
    q_refs, (kv_ref, out_ref, q_ref, kp_ref, vt_ref, score_ref, plan_ref) = refs[:N_X], refs[N_X:]
    for i in range(N_X):
        q_ref[i] = q_refs[i][...]
    lane = iota((TOK, LANES), 1)
    low = lane < HD
    idx = iota((TOK, LANES), 0).astype(F32)

    def doc_of(note):
        n0 = note[0:1, :].astype(F32)
        n1 = note[1:2, :].astype(F32)
        return jnp.where(idx < n0, HD, jnp.where(idx < n1, HD + 1, HD + 2))

    for j in range(N_Z):
        mark = (doc_of(kv_ref[j, TOK:, :]) == lane).astype(F32)
        pair = kv_ref[j, :HALF, :].astype(F32)
        kf = jnp.concatenate([pair, pltpu.roll(pair, HD, 1)], axis=0)
        kp_ref[j * TOK : (j + 1) * TOK, :] = jnp.where(low, kf, mark).astype(BF16)
        vt_ref[j, :HD, :HALF] = kv_ref[j, HALF : HALF + HD, :]
        vt_ref[j, :HD, HALF:] = kv_ref[j, HALF + HD : TOK, :]
        vt_ref[j, HD:, :] = jnp.ones((NOTE, TOK), BF16)

    def documents(note):
        n0, n1 = note[0:1, :].astype(F32), note[1:2, :].astype(F32)
        one = jnp.ones((1, LANES), F32)
        least = jnp.where(n0 <= 0.0, one, 0.0) + jnp.where(n1 <= 0.0, one, 0.0)
        most = jnp.where(n0 < TOK, one, 0.0) + jnp.where(n1 < TOK, one, 0.0)
        return least, most

    ranges = [documents(kv_ref[j, TOK:, :]) for j in range(N_Z)]
    for b in range(N_X):
        least, most = documents(q_ref[b, TOK:, :])
        first = jnp.full((1, LANES), float(N_Z), F32)
        last = jnp.full((1, LANES), -1.0, F32)
        for j, (low_doc, high_doc) in enumerate(ranges):
            meet = (low_doc <= most) & (least <= high_doc)
            first = jnp.where(meet, jnp.minimum(first, float(j)), first)
            last = jnp.where(meet, float(j), last)
        code = jnp.where(last < 0.0, 0.0, first * 16.0 + (last - first + 1.0))
        plan_ref[b] = jnp.max(code).astype(jnp.int32)
    note_row = iota((NOTE, HALF), 0)

    def block(b, start, size):
        qf = q_ref[b, :TOK, :].astype(F32) * (HD**-0.5)
        doc = doc_of(q_ref[b, TOK:, :])
        other = jnp.where((doc == lane) | (lane > HD + 2), 0.0, -MASK_BIG)
        heads = [jnp.where(low, qh, other).astype(BF16) for qh in (qf, pltpu.roll(qf, HD, 1))]
        peaks = [jnp.full((8, TOK), -jnp.inf, F32) for _ in heads]
        accs = [jnp.zeros((HD + NOTE, TOK), F32) for _ in heads]
        tops = [None, None]

        def score(h, j):
            at = pl.multiple_of((start + j) * TOK, TOK)
            part = dot(kp_ref[pl.ds(at, TOK), :], heads[h], 1, 1)
            score_ref[h, j] = part
            peaks[h] = jnp.maximum(peaks[h], jnp.max(part.reshape(TOK // 8, 8, TOK), axis=0))

        def weigh(h, j):
            p = jnp.exp(score_ref[h, j] - tops[h]).astype(BF16)
            accs[h] = accs[h] + dot(vt_ref[start + j], p)

        for j in range(size):
            score(0, j)
        tops[0] = jnp.max(peaks[0], axis=0, keepdims=True)
        for j in range(size):
            score(1, j)
            weigh(0, j)
        tops[1] = jnp.max(peaks[1], axis=0, keepdims=True)
        for j in range(size):
            weigh(1, j)
        peak = jnp.concatenate(tops, axis=1)
        total = jnp.concatenate([acc[HD : HD + 1, :] for acc in accs], axis=1)
        o = [acc[:HD, :] / acc[HD : HD + 1, :] for acc in accs]
        o = jnp.concatenate(o, axis=0).T.astype(BF16)
        terms = split3(peak + jnp.log(total))
        for half in range(2):
            stat = jnp.zeros((NOTE, HALF), F32)
            for i in range(6):
                at = (i // 3) * TOK + half * HALF
                stat = jnp.where(note_row == i, terms[i % 3][:, at : at + HALF], stat)
            to = lax.rem(spot[0] + N_X - b, N_X) * 2 + half
            out_ref[to, :HALF, :] = o[half * HALF : (half + 1) * HALF]
            out_ref[to, HALF:, :] = stat.astype(BF16)

    def step(b, carry):
        code = plan_ref[b]
        first, count = code // 16, code % 16
        fewer = -1
        for size in WINDOWS:

            @pl.when((count > fewer) & (count <= size))
            def _(size=size):
                start = 0 if size == N_Z else jnp.minimum(first, N_Z - size)
                block(b, start, size)

            fewer = size
        return carry

    lax.fori_loop(0, N_X, step, 0)


def project_body(core, in_ref, w_own_ref, w_other_ref, gain_ref, out_ref):
    gain = split3(gain_ref[...])
    row = iota((NOTE, LANES), 0)
    lane = iota((NOTE, LANES), 1)
    pick = (((row < 3) & (lane < HD)) | ((row >= 3) & (row < 6) & (lane >= HD))).astype(BF16)

    def attended(c):
        lse = [dot(in_ref[x * 2 + c, HALF:, :], pick, 0, 0) for x in range(N_X)]
        top = functools.reduce(jnp.maximum, lse)
        total = jnp.zeros((HALF, LANES), F32)
        mixed = jnp.zeros((HALF, LANES), F32)
        for x in range(N_X):
            w = jnp.exp(lse[x] - top)
            total = total + w
            mixed = mixed + w * in_ref[x * 2 + c, :HALF, :].astype(F32)
        return (mixed / total).astype(BF16)

    note = jnp.where(row == 0, gain[0], jnp.where(row == 1, gain[1], jnp.where(row == 2, gain[2], 0.0)))
    own = attended(core[0])
    other = attended(1 - core[0])
    for g in range(N_TP):
        cols = slice(g * LANES, (g + 1) * LANES)
        part = dot(own, w_own_ref[:, cols]) + dot(other, w_other_ref[:, cols])
        out_ref[g, :HALF, :] = part.astype(BF16)
        out_ref[g, HALF:, :] = note.astype(BF16)


def slots_of(routes_ref):
    expert = iota((EXPERTS, TOK), 0)
    r0, r1 = routes_ref[0:1, :], routes_ref[1:2, :]
    named = ((expert == r0) | (expert == r1)).astype(F32)
    before = (iota((TOK, TOK), 0) < iota((TOK, TOK), 1)).astype(BF16)
    slot = dot(named.astype(BF16), before)
    return expert == r0, expert == r1, jnp.where(named > 0.0, slot, -1.0)


def laid_out(slot, value, write):
    slots = iota((CAP_PAD, TOK), 0).astype(F32)
    for e in range(0, EXPERTS, 2):
        both = [jnp.where(slots == slot[i : i + 1, :], value(i), 0.0) for i in (e, e + 1)]
        write(slice(e * CAP_PAD, (e + 2) * CAP_PAD), jnp.concatenate(both, axis=0).astype(BF16))


def route_body(routes_ref, place_ref):
    _, _, slot = slots_of(routes_ref)

    def write(rows, value):
        place_ref[rows, :] = value

    laid_out(slot, lambda e: 1.0, write)


def mix_body(term, routes_ref, weight_ref, mix_ref):
    first, second, slot = slots_of(routes_ref)
    weight = jnp.where(first, weight_ref[0:1, :], jnp.where(second, weight_ref[1:2, :], 0.0))
    part = split3(weight)[term]

    parts = []
    laid_out(slot, lambda e: part[e : e + 1, :], lambda rows, value: parts.append(value))
    for i in range(0, len(parts), 8):
        some = jnp.concatenate(parts[i : i + 8], axis=0).astype(F32)
        mix_ref[:, i * 2 * CAP_PAD : (i + 8) * 2 * CAP_PAD] = some.T.astype(BF16)


def dispatch_body(in_ref, residual_ref, place_ref, mixed_ref, gain_ref, out_ref):
    halves = []
    for c in range(2):
        total = in_ref[c, :HALF, :].astype(F32)
        for y in range(1, N_Y):
            total = total + in_ref[y * 2 + c, :HALF, :].astype(F32)
        halves.append(total)
    for g in range(N_TP):
        note = in_ref[g, HALF:, :].astype(F32)
        gain = note[0:1] + note[1:2] + note[2:3]
        gain_ref[g] = jnp.broadcast_to(gain, (8, LANES))
    mixed = residual_ref[...].astype(F32) + jnp.concatenate(halves, axis=0)
    mixed_ref[...] = mixed
    out_ref[...] = dot(place_ref[...], mixed.astype(BF16)).astype(BF16)


def spread_body(in_ref, drop_ref, out_ref):
    span = BLOCKS * CAP_PAD
    for r in range(GROUPS):
        kept = dot(drop_ref[...], in_ref[r * span : (r + 1) * span, :]).astype(BF16)
        for g in range(r, N_TP, GROUPS):
            out_ref[g] = kept


def expert_body(in_ref, gain_ref, late_ref, *refs):
    many = 3 * GROUPS - 1
    far, (out_ref, x_ref), weights, sems = refs[:many], refs[many : many + 2], refs[many + 2 : -1], refs[-1]
    copies = [pltpu.make_async_copy(far[i], weights[i], sems.at[i]) for i in range(many)]
    for copy in copies:
        copy.start()
    total = jnp.zeros((ROWS, LANES), F32)
    for g in range(N_TP):
        x = in_ref[g].astype(F32)
        total = total + x * x
    scale = lax.rsqrt(jnp.sum(total, axis=1, keepdims=True) * (1.0 / D) + EPSILON)
    for g in range(N_TP):
        x = in_ref[g].astype(F32) * scale * gain_ref[g, 0:1, :]
        x_ref[:, g * LANES : (g + 1) * LANES] = x.astype(BF16)
    hidden = []
    for i in range(GROUPS):
        copies[2 * i].wait()
        gate = jnp.minimum(dot(x_ref[...], weights[2 * i][...]), CLAMP_LIMIT)
        copies[2 * i + 1].wait()
        up = jnp.clip(dot(x_ref[...], weights[2 * i + 1][...]), -CLAMP_LIMIT, CLAMP_LIMIT)
        unit = gate * (1.0 / (1.0 + jnp.exp(-SIGMOID_SCALE * gate))) * (up + 1.0)
        hidden.append(unit.astype(BF16))
    for copy in copies[2 * GROUPS :]:
        copy.wait()
    downs = weights[2 * GROUPS :] + (late_ref,)
    for g in range(0, N_TP, 2):
        cols = slice(g * LANES, (g + 2) * LANES)
        part = dot(hidden[0], downs[0][:, cols])
        for h, w in zip(hidden[1:], downs[1:]):
            part = part + dot(h, w[:, cols])
        part = part.astype(BF16)
        out_ref[g] = part[:, :LANES]
        out_ref[g + 1] = part[:, LANES:]


def gather_body(in_ref, widen_ref, out_ref):
    span = BLOCKS * CAP_PAD
    for r in range(GROUPS):
        total = in_ref[r].astype(F32)
        for g in range(r + GROUPS, N_TP, GROUPS):
            total = total + in_ref[g].astype(F32)
        rows = dot(widen_ref[...], total.astype(BF16)).astype(BF16)
        out_ref[r * span : (r + 1) * span, :] = rows


def finish_body(in_ref, mix0_ref, mix1_ref, mix2_ref, mixed_ref, out_ref):
    total = mixed_ref[...]
    rows = in_ref[...]
    for mix_ref in (mix0_ref, mix1_ref, mix2_ref):
        total = total + dot(mix_ref[...], rows)
    out_ref[...] = total.astype(BF16)


def shaped(shape, dtype=BF16):
    return pltpu.VMEM(shape, dtype)


VMEM = pl.BlockSpec(memory_space=pltpu.VMEM)
SMEM = pl.BlockSpec(memory_space=pltpu.SMEM)
HBM = pl.BlockSpec(memory_space=pltpu.HBM)


def call(body, outs, *args, scratch=(), mib=8, far=0):
    near = len(args) - far
    specs = [SMEM if a.shape == (1,) else VMEM for a in args[:near]] + [HBM] * far
    args = args[:near] + tuple(pltpu.with_memory_space_constraint(a, pltpu.HBM) for a in args[near:])
    many = isinstance(outs, (list, tuple))
    return pl.pallas_call(
        body,
        out_shape=outs,
        in_specs=specs,
        out_specs=[VMEM] * len(outs) if many else VMEM,
        scratch_shapes=list(scratch),
        compiler_params=pltpu.CompilerParams(vmem_limit_bytes=mib * 1024 * 1024),
    )(*args)


def exchange(x, axes):
    return lax.all_to_all(x, axes, 0, 0, tiled=True)


def shifted(x, axis, size, by):
    return lax.ppermute(x, axis, [(i, (i + by) % size) for i in range(size)])


def partner(x):
    return lax.ppermute(x, "c", [(0, 1), (1, 0)])


def neighbour(x):
    return lax.ppermute(x, "y", [(i, i ^ 1) for i in range(N_Y)])


def per_device(
    queries,
    keys,
    values,
    docs,
    query_gain,
    key_gain,
    out_weight,
    residual,
    norm_gain,
    routes,
    route_weight,
    gate_weight,
    up_weight,
    down_weight,
):
    return step(
        queries,
        keys.T,
        values.T,
        docs.reshape(2, LANES),
        query_gain.reshape(1, HD),
        key_gain.reshape(1, HD),
        out_weight,
        residual,
        norm_gain,
        routes.T,
        route_weight.T,
        gate_weight[0],
        up_weight[0],
        down_weight[0],
    )


def step(
    queries,
    keys,
    values,
    docs,
    query_gain,
    key_gain,
    out_weight,
    residual,
    norm_gain,
    routes,
    route_weight,
    gate,
    up,
    down,
):
    row_tab, col_tab = tables()
    drop = compaction()
    block = (lax.axis_index("z") * N_X + lax.axis_index("x")).reshape(1).astype(jnp.int32)
    spot = lax.axis_index("x").reshape(1).astype(jnp.int32)
    core = lax.axis_index("c").reshape(1).astype(jnp.int32)
    sources = (
        queries,
        keys,
        values,
        docs,
        query_gain,
        key_gain,
        jnp.asarray(row_tab),
        jnp.asarray(col_tab),
    )
    kept = [pltpu.VMEM(a.shape[1:] if i == 6 else a.shape, a.dtype) for i, a in enumerate(sources)]
    qs, kvs = call(
        prep_body,
        [shaped((TOK + NOTE, LANES)), shaped((N_Z, TOK + NOTE, LANES))],
        block,
        *sources,
        scratch=kept + [pltpu.SemaphoreType.DMA((len(sources),))],
        far=len(sources),
    )
    kv_all = exchange(kvs, "z")
    q_all = [qs] + [shifted(qs, "x", N_X, i) for i in range(1, N_X)]
    out_other = partner(out_weight)
    gate_y, up_y = neighbour(gate), neighbour(up)
    down_y = neighbour(down)
    gate_o, up_o = partner(gate), partner(up)
    down_o = partner(down)
    gate_yo, up_yo = partner(gate_y), partner(up_y)
    down_yo = partner(down_y)
    slot_table = shaped((EXPERTS * CAP_PAD, TOK))
    mix_table = shaped((TOK, EXPERTS * CAP_PAD))
    place = call(route_body, slot_table, routes)
    mixes = [
        call(functools.partial(mix_body, i), mix_table, routes, route_weight)
        for i in range(3)
    ]
    partial = call(
        attend_body,
        shaped((N_X * 2, HALF + NOTE, LANES)),
        spot,
        *q_all,
        kv_all,
        scratch=[
            pltpu.VMEM((N_X, TOK + NOTE, LANES), BF16),
            pltpu.VMEM((N_Z * TOK, LANES), BF16),
            pltpu.VMEM((N_Z, HD + NOTE, TOK), BF16),
            pltpu.VMEM((2, N_Z, TOK, TOK), F32),
            pltpu.SMEM((N_X,), jnp.int32),
        ],
        mib=24,
    )
    partial = exchange(partial, ("x", "c"))
    projected = call(
        project_body,
        shaped((N_TP, HALF + NOTE, LANES)),
        core,
        partial,
        out_weight,
        out_other,
        norm_gain.reshape(1, LANES),
    )
    projected = exchange(projected, ("y", "c"))
    mixed, gain_all, outgoing = call(
        dispatch_body,
        [
            shaped((TOK, LANES), F32),
            shaped((N_TP, 8, LANES), F32),
            shaped((EXPERTS * CAP_PAD, LANES)),
        ],
        projected,
        residual,
        place,
    )
    arrived = exchange(outgoing.reshape(N_SP, CAP_PAD, LANES), ("z", "x"))
    spread = call(
        spread_body,
        shaped((N_TP, ROWS, LANES)),
        arrived.reshape(N_SP * CAP_PAD, LANES),
        jnp.asarray(drop, BF16),
    )
    columns = exchange(spread, ("y", "c"))
    weights = (gate, up, gate_o, up_o, gate_y, up_y, gate_yo, up_yo, down, down_o, down_y)
    parts = call(
        expert_body,
        shaped((N_TP, ROWS, LANES)),
        columns,
        gain_all,
        down_yo,
        *weights,
        scratch=[pltpu.VMEM((ROWS, D), BF16)]
        + [pltpu.VMEM(w.shape, BF16) for w in weights]
        + [pltpu.SemaphoreType.DMA((len(weights),))],
        mib=32,
        far=len(weights),
    )
    parts = exchange(parts, ("y", "c"))
    expert_out = call(
        gather_body, shaped((N_SP * CAP_PAD, LANES)), parts, jnp.asarray(drop.T, BF16)
    )
    returned = exchange(expert_out.reshape(N_SP, CAP_PAD, LANES), ("z", "x"))
    return call(
        finish_body,
        jax.ShapeDtypeStruct((TOK, LANES), BF16),
        returned.reshape(N_SP * CAP_PAD, LANES),
        *mixes,
        mixed,
    )


def solution(mesh):
    grid = Mesh(mesh.devices.reshape(N_Z, N_X, N_Y, N_C), ("z", "x", "y", "c"))
    sp, tp = ("z", "x"), ("y", "c")
    in_specs = (
        P(sp, tp),
        P(sp, tp),
        P(sp, tp),
        P(sp),
        P(),
        P(),
        P(tp, None),
        P(sp, tp),
        P(tp),
        P(sp, None),
        P(sp, None),
        P(sp, None, tp),
        P(sp, None, tp),
        P(sp, tp, None),
    )
    return jax.shard_map(
        per_device, mesh=grid, in_specs=in_specs, out_specs=P(sp, tp), check_vma=False
    )
```

```python
import functools

import jax
import jax.numpy as jnp
import numpy as np
from jax import lax
from jax.experimental import pallas as pl
from jax.experimental.pallas import tpu as pltpu
from jax.sharding import Mesh, PartitionSpec as P


GRID_W = 64
EPSILON = 1e-06
ROTARY_BASE = 10000.0
CLAMP_LIMIT = 7.0
SIGMOID_SCALE = 1.702
N_Z, N_X, N_Y, N_C = 8, 4, 8, 2
N_SP, N_TP = N_Z * N_X, N_Y * N_C
TOK = 256
HALF = TOK // 2
HD = 64
LANES = 128
D = 2048
EXPERTS = 32
CAP = 20
CAP_PAD = 24
GROUPS = 4
ROWS = N_SP * CAP // GROUPS
BLOCKS = N_SP // GROUPS
NOTE = 16
MASK_BIG = 16384.0
WINDOWS = (5, 6, N_Z)

F32 = jnp.float32
BF16 = jnp.bfloat16


def tables():
    quarter = HD // 4
    freqs = (ROTARY_BASE ** (-np.arange(quarter, dtype=np.float32) / quarter)).astype(np.float32)
    lane = np.arange(LANES)
    pair = (lane % HD) // 2
    is_row = pair < quarter
    freq = freqs[np.where(is_row, pair, pair - quarter)]
    sign = np.where(lane % 2 == 0, -1.0, 1.0)
    cols = (np.arange(GRID_W, dtype=np.float32)[:, None] * freq).astype(np.float32)
    rows = (np.arange(N_SP * TOK // GRID_W, dtype=np.float32)[:, None] * freq).astype(np.float32)
    cols, rows = cols.astype(np.float64), rows.astype(np.float64)
    keep = lambda a, m: np.where(m, a, 0.0).astype(np.float32)
    per = TOK // GRID_W
    row_c = keep(np.cos(rows), is_row).reshape(N_SP, per, LANES)
    row_s = keep(np.sin(rows) * sign, is_row).reshape(N_SP, per, LANES)
    row_tab = np.concatenate([row_c, row_s], axis=1)
    col_tab = np.stack([keep(np.cos(cols), ~is_row), keep(np.sin(cols) * sign, ~is_row)])
    return row_tab, col_tab


def compaction():
    out = np.zeros((ROWS, BLOCKS * CAP_PAD), np.float32)
    r = np.arange(ROWS)
    out[r, (r // CAP) * CAP_PAD + r % CAP] = 1.0
    return out


def dot(a, b, ca=1, cb=0):
    return lax.dot_general(a, b, (((ca,), (cb,)), ((), ())), preferred_element_type=F32)


def iota(shape, dim):
    return lax.broadcasted_iota(jnp.int32, shape, dim)


def prep_body(blk, *refs):
    sources, (qs_ref, kvs_ref, gain_ref), kept, sems = refs[:9], refs[9:12], refs[12:21], refs[21]
    copies = []
    for i, (src, dst) in enumerate(zip(sources, kept)):
        src = src.at[blk[0]] if i == 6 else src
        copies.append(pltpu.make_async_copy(src, dst, sems.at[i]))
    for copy in copies:
        copy.start()
    for copy in copies:
        copy.wait()
    q_ref, k_ref, v_ref, docs_ref, qg_ref, kg_ref, row_ref, col_ref, norm_ref = kept
    gain_ref[...] = norm_ref[...]
    lane = iota((TOK, LANES), 1)
    low = lane < HD
    even = (lane & 1) == 0
    rows = row_ref[...]
    per = TOK // GRID_W
    cos_t = jnp.concatenate([col_ref[0] + rows[j : j + 1] for j in range(per)], axis=0)
    sin_t = jnp.concatenate([col_ref[1] + rows[per + j : per + j + 1] for j in range(per)], axis=0)

    def turn(n):
        swapped = jnp.where(even, pltpu.roll(n, LANES - 1, 1), pltpu.roll(n, 1, 1))
        return n * cos_t + swapped * sin_t

    x = q_ref[...].astype(F32)
    sq = x * x
    s0 = jnp.sum(jnp.where(low, sq, 0.0), axis=1, keepdims=True)
    s1 = jnp.sum(jnp.where(low, 0.0, sq), axis=1, keepdims=True)
    r0 = lax.rsqrt(s0 * (1.0 / HD) + EPSILON)
    r1 = lax.rsqrt(s1 * (1.0 / HD) + EPSILON)
    gain = jnp.concatenate([qg_ref[...], qg_ref[...]], axis=1)
    q_out = turn(x * jnp.where(low, r0, r1) * gain).astype(BF16)

    flat = k_ref[...].astype(F32)
    k = jnp.concatenate([flat, jnp.zeros_like(flat)], axis=0).T
    rk = lax.rsqrt(jnp.sum(k * k, axis=1, keepdims=True) * (1.0 / HD) + EPSILON)
    gain_k = jnp.concatenate([kg_ref[...], kg_ref[...]], axis=1)
    k = turn(k * rk * gain_k)
    keys = jnp.where(low[:HALF], k[:HALF], pltpu.roll(k[HALF:], HD, 1)).astype(BF16)
    values = v_ref[...]

    docs = docs_ref[...]
    n0 = jnp.sum((docs < 1).astype(F32))
    n1 = jnp.sum((docs < 2).astype(F32))
    row = iota((NOTE, LANES), 0)
    note = jnp.where(row == 0, n0, jnp.where(row == 1, n1, 0.0)).astype(BF16)
    qs_ref[:TOK, :] = q_out
    qs_ref[TOK:, :] = note
    for i in range(N_Z):
        kvs_ref[i, :HALF, :] = keys
        kvs_ref[i, HALF : HALF + HD, :] = values[:, :HALF]
        kvs_ref[i, HALF + HD : TOK, :] = values[:, HALF:]
        kvs_ref[i, TOK:, :] = note


def split3(x):
    hi = x.astype(BF16).astype(F32)
    mid = (x - hi).astype(BF16).astype(F32)
    return hi, mid, x - hi - mid


def attend_body(spot, *refs):
    q_refs, (kv_ref, out_ref, q_ref, kp_ref, vt_ref, score_ref, plan_ref) = refs[:N_X], refs[N_X:]
    for i in range(N_X):
        q_ref[i] = q_refs[i][...]
    lane = iota((TOK, LANES), 1)
    low = lane < HD
    idx = iota((TOK, LANES), 0).astype(F32)

    def doc_of(note):
        n0 = note[0:1, :].astype(F32)
        n1 = note[1:2, :].astype(F32)
        return jnp.where(idx < n0, HD, jnp.where(idx < n1, HD + 1, HD + 2))

    for j in range(N_Z):
        mark = (doc_of(kv_ref[j, TOK:, :]) == lane).astype(F32)
        pair = kv_ref[j, :HALF, :].astype(F32)
        kf = jnp.concatenate([pair, pltpu.roll(pair, HD, 1)], axis=0)
        kp_ref[j * TOK : (j + 1) * TOK, :] = jnp.where(low, kf, mark).astype(BF16)
        vt_ref[j, :HD, :HALF] = kv_ref[j, HALF : HALF + HD, :]
        vt_ref[j, :HD, HALF:] = kv_ref[j, HALF + HD : TOK, :]
        vt_ref[j, HD:, :] = jnp.ones((NOTE, TOK), BF16)

    def documents(note):
        n0, n1 = note[0:1, :].astype(F32), note[1:2, :].astype(F32)
        one = jnp.ones((1, LANES), F32)
        least = jnp.where(n0 <= 0.0, one, 0.0) + jnp.where(n1 <= 0.0, one, 0.0)
        most = jnp.where(n0 < TOK, one, 0.0) + jnp.where(n1 < TOK, one, 0.0)
        return least, most

    ranges = [documents(kv_ref[j, TOK:, :]) for j in range(N_Z)]
    for b in range(N_X):
        least, most = documents(q_ref[b, TOK:, :])
        first = jnp.full((1, LANES), float(N_Z), F32)
        last = jnp.full((1, LANES), -1.0, F32)
        for j, (low_doc, high_doc) in enumerate(ranges):
            meet = (low_doc <= most) & (least <= high_doc)
            first = jnp.where(meet, jnp.minimum(first, float(j)), first)
            last = jnp.where(meet, float(j), last)
        code = jnp.where(last < 0.0, 0.0, first * 16.0 + (last - first + 1.0))
        plan_ref[b] = jnp.max(code).astype(jnp.int32)
    note_row = iota((NOTE, HALF), 0)

    def block(b, start, size):
        qf = q_ref[b, :TOK, :].astype(F32) * (HD**-0.5)
        doc = doc_of(q_ref[b, TOK:, :])
        other = jnp.where((doc == lane) | (lane > HD + 2), 0.0, -MASK_BIG)
        heads = [jnp.where(low, qh, other).astype(BF16) for qh in (qf, pltpu.roll(qf, HD, 1))]
        peaks = [jnp.full((8, TOK), -jnp.inf, F32) for _ in heads]
        accs = [jnp.zeros((HD + NOTE, TOK), F32) for _ in heads]
        tops = [None, None]

        def score(h, j):
            at = pl.multiple_of((start + j) * TOK, TOK)
            part = dot(kp_ref[pl.ds(at, TOK), :], heads[h], 1, 1)
            score_ref[h, j] = part
            peaks[h] = jnp.maximum(peaks[h], jnp.max(part.reshape(TOK // 8, 8, TOK), axis=0))

        def weigh(h, j):
            p = jnp.exp(score_ref[h, j] - tops[h]).astype(BF16)
            accs[h] = accs[h] + dot(vt_ref[start + j], p)

        for j in range(size):
            score(0, j)
        tops[0] = jnp.max(peaks[0], axis=0, keepdims=True)
        for j in range(size):
            score(1, j)
            weigh(0, j)
        tops[1] = jnp.max(peaks[1], axis=0, keepdims=True)
        for j in range(size):
            weigh(1, j)
        peak = jnp.concatenate(tops, axis=1)
        total = jnp.concatenate([acc[HD : HD + 1, :] for acc in accs], axis=1)
        o = [acc[:HD, :] / acc[HD : HD + 1, :] for acc in accs]
        o = jnp.concatenate(o, axis=0).T.astype(BF16)
        terms = split3(peak + jnp.log(total))
        for half in range(2):
            stat = jnp.zeros((NOTE, HALF), F32)
            for i in range(6):
                at = (i // 3) * TOK + half * HALF
                stat = jnp.where(note_row == i, terms[i % 3][:, at : at + HALF], stat)
            to = lax.rem(spot[0] + N_X - b, N_X) * 2 + half
            out_ref[to, :HALF, :] = o[half * HALF : (half + 1) * HALF]
            out_ref[to, HALF:, :] = stat.astype(BF16)

    def step(b, carry):
        code = plan_ref[b]
        first, count = code // 16, code % 16
        fewer = -1
        for size in WINDOWS:

            @pl.when((count > fewer) & (count <= size))
            def _(size=size):
                start = 0 if size == N_Z else jnp.minimum(first, N_Z - size)
                block(b, start, size)

            fewer = size
        return carry

    lax.fori_loop(0, N_X, step, 0)


def project_body(core, in_ref, w_own_ref, w_other_ref, gain_ref, out_ref):
    gain = split3(gain_ref[...])
    row = iota((NOTE, LANES), 0)
    lane = iota((NOTE, LANES), 1)
    pick = (((row < 3) & (lane < HD)) | ((row >= 3) & (row < 6) & (lane >= HD))).astype(BF16)

    def attended(c):
        lse = [dot(in_ref[x * 2 + c, HALF:, :], pick, 0, 0) for x in range(N_X)]
        top = functools.reduce(jnp.maximum, lse)
        total = jnp.zeros((HALF, LANES), F32)
        mixed = jnp.zeros((HALF, LANES), F32)
        for x in range(N_X):
            w = jnp.exp(lse[x] - top)
            total = total + w
            mixed = mixed + w * in_ref[x * 2 + c, :HALF, :].astype(F32)
        return (mixed / total).astype(BF16)

    note = jnp.where(row == 0, gain[0], jnp.where(row == 1, gain[1], jnp.where(row == 2, gain[2], 0.0)))
    own = attended(core[0])
    other = attended(1 - core[0])
    for g in range(N_TP):
        cols = slice(g * LANES, (g + 1) * LANES)
        part = dot(own, w_own_ref[:, cols]) + dot(other, w_other_ref[:, cols])
        out_ref[g, :HALF, :] = part.astype(BF16)
        out_ref[g, HALF:, :] = note.astype(BF16)


def slots_of(routes_ref):
    expert = iota((EXPERTS, TOK), 0)
    r0, r1 = routes_ref[0:1, :], routes_ref[1:2, :]
    named = ((expert == r0) | (expert == r1)).astype(F32)
    before = (iota((TOK, TOK), 0) < iota((TOK, TOK), 1)).astype(BF16)
    slot = dot(named.astype(BF16), before)
    return expert == r0, expert == r1, jnp.where(named > 0.0, slot, -1.0)


def laid_out(slot, value, write):
    slots = iota((CAP_PAD, TOK), 0).astype(F32)
    for e in range(0, EXPERTS, 2):
        both = [jnp.where(slots == slot[i : i + 1, :], value(i), 0.0) for i in (e, e + 1)]
        write(slice(e * CAP_PAD, (e + 2) * CAP_PAD), jnp.concatenate(both, axis=0).astype(BF16))


def route_body(routes_ref, place_ref):
    _, _, slot = slots_of(routes_ref)

    def write(rows, value):
        place_ref[rows, :] = value

    laid_out(slot, lambda e: 1.0, write)


def mix_body(term, routes_ref, weight_ref, mix_ref):
    first, second, slot = slots_of(routes_ref)
    weight = jnp.where(first, weight_ref[0:1, :], jnp.where(second, weight_ref[1:2, :], 0.0))
    part = split3(weight)[term]

    parts = []
    laid_out(slot, lambda e: part[e : e + 1, :], lambda rows, value: parts.append(value))
    for i in range(0, len(parts), 8):
        some = jnp.concatenate(parts[i : i + 8], axis=0).astype(F32)
        mix_ref[:, i * 2 * CAP_PAD : (i + 8) * 2 * CAP_PAD] = some.T.astype(BF16)


def dispatch_body(in_ref, residual_ref, place_ref, mixed_ref, gain_ref, out_ref):
    halves = []
    for c in range(2):
        total = in_ref[c, :HALF, :].astype(F32)
        for y in range(1, N_Y):
            total = total + in_ref[y * 2 + c, :HALF, :].astype(F32)
        halves.append(total)
    for g in range(N_TP):
        note = in_ref[g, HALF:, :].astype(F32)
        gain = note[0:1] + note[1:2] + note[2:3]
        gain_ref[g] = jnp.broadcast_to(gain, (8, LANES))
    mixed = residual_ref[...].astype(F32) + jnp.concatenate(halves, axis=0)
    mixed_ref[...] = mixed
    out_ref[...] = dot(place_ref[...], mixed.astype(BF16)).astype(BF16)


def spread_body(in_ref, drop_ref, out_ref):
    span = BLOCKS * CAP_PAD
    for r in range(GROUPS):
        kept = dot(drop_ref[...], in_ref[r * span : (r + 1) * span, :]).astype(BF16)
        for g in range(r, N_TP, GROUPS):
            out_ref[g] = kept


def expert_body(in_ref, gain_ref, late_ref, *refs):
    many = 3 * GROUPS - 1
    far, (out_ref, x_ref), weights, sems = refs[:many], refs[many : many + 2], refs[many + 2 : -1], refs[-1]
    copies = [pltpu.make_async_copy(far[i], weights[i], sems.at[i]) for i in range(many)]
    for copy in copies[:4]:
        copy.start()
    total = jnp.zeros((ROWS, LANES), F32)
    for g in range(N_TP):
        x = in_ref[g].astype(F32)
        total = total + x * x
    scale = lax.rsqrt(jnp.sum(total, axis=1, keepdims=True) * (1.0 / D) + EPSILON)
    for g in range(N_TP):
        x = in_ref[g].astype(F32) * scale * gain_ref[g, 0:1, :]
        x_ref[:, g * LANES : (g + 1) * LANES] = x.astype(BF16)
    hidden = []
    for i in range(GROUPS):
        copies[2 * i].wait()
        copies[2 * i + 1].wait()
        for copy in copies[2 * i + 4 : 2 * i + 6]:
            copy.start()
        gate = jnp.minimum(dot(x_ref[...], weights[2 * i][...]), CLAMP_LIMIT)
        up = jnp.clip(dot(x_ref[...], weights[2 * i + 1][...]), -CLAMP_LIMIT, CLAMP_LIMIT)
        unit = gate * (1.0 / (1.0 + jnp.exp(-SIGMOID_SCALE * gate))) * (up + 1.0)
        hidden.append(unit.astype(BF16))
    for copy in copies[2 * GROUPS :]:
        copy.wait()
    downs = weights[2 * GROUPS :] + (late_ref,)
    for g in range(0, N_TP, 2):
        cols = slice(g * LANES, (g + 2) * LANES)
        part = dot(hidden[0], downs[0][:, cols])
        for h, w in zip(hidden[1:], downs[1:]):
            part = part + dot(h, w[:, cols])
        part = part.astype(BF16)
        out_ref[g] = part[:, :LANES]
        out_ref[g + 1] = part[:, LANES:]


def gather_body(in_ref, widen_ref, out_ref):
    span = BLOCKS * CAP_PAD
    for r in range(GROUPS):
        total = in_ref[r].astype(F32)
        for g in range(r + GROUPS, N_TP, GROUPS):
            total = total + in_ref[g].astype(F32)
        rows = dot(widen_ref[...], total.astype(BF16)).astype(BF16)
        out_ref[r * span : (r + 1) * span, :] = rows


def finish_body(in_ref, mix0_ref, mix1_ref, mix2_ref, mixed_ref, out_ref):
    total = mixed_ref[...]
    rows = in_ref[...]
    for mix_ref in (mix0_ref, mix1_ref, mix2_ref):
        total = total + dot(mix_ref[...], rows)
    out_ref[...] = total.astype(BF16)


def shaped(shape, dtype=BF16):
    return pltpu.VMEM(shape, dtype)


VMEM = pl.BlockSpec(memory_space=pltpu.VMEM)
SMEM = pl.BlockSpec(memory_space=pltpu.SMEM)
HBM = pl.BlockSpec(memory_space=pltpu.HBM)


def call(body, outs, *args, scratch=(), mib=8, far=0):
    near = len(args) - far
    specs = [SMEM if a.shape == (1,) else VMEM for a in args[:near]] + [HBM] * far
    args = args[:near] + tuple(pltpu.with_memory_space_constraint(a, pltpu.HBM) for a in args[near:])
    many = isinstance(outs, (list, tuple))
    return pl.pallas_call(
        body,
        out_shape=outs,
        in_specs=specs,
        out_specs=[VMEM] * len(outs) if many else VMEM,
        scratch_shapes=list(scratch),
        compiler_params=pltpu.CompilerParams(vmem_limit_bytes=mib * 1024 * 1024),
    )(*args)


def exchange(x, axes):
    return lax.all_to_all(x, axes, 0, 0, tiled=True)


def shifted(x, axis, size, by):
    return lax.ppermute(x, axis, [(i, (i + by) % size) for i in range(size)])


def partner(x):
    return lax.ppermute(x, "c", [(0, 1), (1, 0)])


def neighbour(x):
    pairs = []
    for y in range(N_Y):
        for c, to in ((0, y ^ 1), (1, (((y + 1) ^ 1) - 1) % N_Y)):
            pairs.append((y * N_C + c, to * N_C + c))
    return lax.ppermute(x, ("y", "c"), pairs)


def per_device(
    queries,
    keys,
    values,
    docs,
    query_gain,
    key_gain,
    out_weight,
    residual,
    norm_gain,
    routes,
    route_weight,
    gate_weight,
    up_weight,
    down_weight,
):
    return step(
        queries,
        keys.T,
        values.T,
        docs.reshape(2, LANES),
        query_gain.reshape(1, HD),
        key_gain.reshape(1, HD),
        out_weight,
        residual,
        norm_gain,
        routes.T,
        route_weight.T,
        gate_weight[0],
        up_weight[0],
        down_weight[0],
    )


def step(
    queries,
    keys,
    values,
    docs,
    query_gain,
    key_gain,
    out_weight,
    residual,
    norm_gain,
    routes,
    route_weight,
    gate,
    up,
    down,
):
    row_tab, col_tab = tables()
    drop = compaction()
    block = (lax.axis_index("z") * N_X + lax.axis_index("x")).reshape(1).astype(jnp.int32)
    spot = lax.axis_index("x").reshape(1).astype(jnp.int32)
    core = lax.axis_index("c").reshape(1).astype(jnp.int32)
    sources = (
        queries,
        keys,
        values,
        docs,
        query_gain,
        key_gain,
        jnp.asarray(row_tab),
        jnp.asarray(col_tab),
        norm_gain.reshape(1, LANES),
    )
    kept = [pltpu.VMEM(a.shape[1:] if i == 6 else a.shape, a.dtype) for i, a in enumerate(sources)]
    qs, kvs, gain_own = call(
        prep_body,
        [
            shaped((TOK + NOTE, LANES)),
            shaped((N_Z, TOK + NOTE, LANES)),
            shaped((1, LANES), F32),
        ],
        block,
        *sources,
        scratch=kept + [pltpu.SemaphoreType.DMA((len(sources),))],
        far=len(sources),
    )
    kv_all = exchange(kvs, "z")
    q_all = [qs] + [shifted(qs, "x", N_X, i) for i in range(1, N_X)]
    out_other = partner(out_weight)
    gate_y, up_y = neighbour(gate), neighbour(up)
    down_y = neighbour(down)
    gate_o, up_o = partner(gate), partner(up)
    down_o = partner(down)
    gate_yo, up_yo = partner(gate_y), partner(up_y)
    down_yo = partner(down_y)
    slot_table = shaped((EXPERTS * CAP_PAD, TOK))
    mix_table = shaped((TOK, EXPERTS * CAP_PAD))
    place = call(route_body, slot_table, routes)
    mixes = [
        call(functools.partial(mix_body, i), mix_table, routes, route_weight)
        for i in range(3)
    ]
    partial = call(
        attend_body,
        shaped((N_X * 2, HALF + NOTE, LANES)),
        spot,
        *q_all,
        kv_all,
        scratch=[
            pltpu.VMEM((N_X, TOK + NOTE, LANES), BF16),
            pltpu.VMEM((N_Z * TOK, LANES), BF16),
            pltpu.VMEM((N_Z, HD + NOTE, TOK), BF16),
            pltpu.VMEM((2, N_Z, TOK, TOK), F32),
            pltpu.SMEM((N_X,), jnp.int32),
        ],
        mib=24,
    )
    partial = exchange(partial, ("x", "c"))
    projected = call(
        project_body,
        shaped((N_TP, HALF + NOTE, LANES)),
        core,
        partial,
        out_weight,
        out_other,
        gain_own,
    )
    projected = exchange(projected, ("y", "c"))
    mixed, gain_all, outgoing = call(
        dispatch_body,
        [
            shaped((TOK, LANES), F32),
            shaped((N_TP, 8, LANES), F32),
            shaped((EXPERTS * CAP_PAD, LANES)),
        ],
        projected,
        residual,
        place,
    )
    arrived = exchange(outgoing.reshape(N_SP, CAP_PAD, LANES), ("z", "x"))
    spread = call(
        spread_body,
        shaped((N_TP, ROWS, LANES)),
        arrived.reshape(N_SP * CAP_PAD, LANES),
        jnp.asarray(drop, BF16),
    )
    columns = exchange(spread, ("y", "c"))
    weights = (gate, up, gate_o, up_o, gate_y, up_y, gate_yo, up_yo, down, down_o, down_y)
    parts = call(
        expert_body,
        shaped((N_TP, ROWS, LANES)),
        columns,
        gain_all,
        down_yo,
        *weights,
        scratch=[pltpu.VMEM((ROWS, D), BF16)]
        + [pltpu.VMEM(w.shape, BF16) for w in weights]
        + [pltpu.SemaphoreType.DMA((len(weights),))],
        mib=32,
        far=len(weights),
    )
    parts = exchange(parts, ("y", "c"))
    expert_out = call(
        gather_body, shaped((N_SP * CAP_PAD, LANES)), parts, jnp.asarray(drop.T, BF16)
    )
    returned = exchange(expert_out.reshape(N_SP, CAP_PAD, LANES), ("z", "x"))
    return call(
        finish_body,
        jax.ShapeDtypeStruct((TOK, LANES), BF16),
        returned.reshape(N_SP * CAP_PAD, LANES),
        *mixes,
        mixed,
    )


def solution(mesh):
    grid = Mesh(mesh.devices.reshape(N_Z, N_X, N_Y, N_C), ("z", "x", "y", "c"))
    sp, tp = ("z", "x"), ("y", "c")
    in_specs = (
        P(sp, tp),
        P(sp, tp),
        P(sp, tp),
        P(sp),
        P(),
        P(),
        P(tp, None),
        P(sp, tp),
        P(tp),
        P(sp, None),
        P(sp, None),
        P(sp, None, tp),
        P(sp, None, tp),
        P(sp, tp, None),
    )
    return jax.shard_map(
        per_device, mesh=grid, in_specs=in_specs, out_specs=P(sp, tp), check_vma=False
    )
```

```python
import functools

import jax
import jax.numpy as jnp
import numpy as np
from jax import lax
from jax.experimental import pallas as pl
from jax.experimental.pallas import tpu as pltpu
from jax.sharding import Mesh, PartitionSpec as P


GRID_W = 64
EPSILON = 1e-06
ROTARY_BASE = 10000.0
CLAMP_LIMIT = 7.0
SIGMOID_SCALE = 1.702
N_Z, N_X, N_Y, N_C = 8, 4, 8, 2
N_SP, N_TP = N_Z * N_X, N_Y * N_C
TOK = 256
HALF = TOK // 2
HD = 64
LANES = 128
D = 2048
EXPERTS = 32
CAP = 20
CAP_PAD = 24
GROUPS = 4
ROWS = N_SP * CAP // GROUPS
BLOCKS = N_SP // GROUPS
NOTE = 8
SUMS = 16
MASK_BIG = 16384.0
WINDOWS = (5, 6, N_Z)

F32 = jnp.float32
BF16 = jnp.bfloat16


def tables():
    quarter = HD // 4
    freqs = (ROTARY_BASE ** (-np.arange(quarter, dtype=np.float32) / quarter)).astype(np.float32)
    lane = np.arange(LANES)
    pair = (lane % HD) // 2
    is_row = pair < quarter
    freq = freqs[np.where(is_row, pair, pair - quarter)]
    sign = np.where(lane % 2 == 0, -1.0, 1.0)
    cols = (np.arange(GRID_W, dtype=np.float32)[:, None] * freq).astype(np.float32)
    rows = (np.arange(N_SP * TOK // GRID_W, dtype=np.float32)[:, None] * freq).astype(np.float32)
    cols, rows = cols.astype(np.float64), rows.astype(np.float64)
    keep = lambda a, m: np.where(m, a, 0.0).astype(np.float32)
    per = TOK // GRID_W
    row_c = keep(np.cos(rows), is_row).reshape(N_SP, per, LANES)
    row_s = keep(np.sin(rows) * sign, is_row).reshape(N_SP, per, LANES)
    row_tab = np.concatenate([row_c, row_s], axis=1)
    col_tab = np.stack([keep(np.cos(cols), ~is_row), keep(np.sin(cols) * sign, ~is_row)])
    return row_tab, col_tab


def compaction():
    out = np.zeros((ROWS, BLOCKS * CAP_PAD), np.float32)
    r = np.arange(ROWS)
    out[r, (r // CAP) * CAP_PAD + r % CAP] = 1.0
    return out


def dot(a, b, ca=1, cb=0):
    return lax.dot_general(a, b, (((ca,), (cb,)), ((), ())), preferred_element_type=F32)


def iota(shape, dim):
    return lax.broadcasted_iota(jnp.int32, shape, dim)


def prep_body(blk, *refs):
    sources, (qs_ref, kvs_ref, gain_ref), kept, sems = refs[:9], refs[9:12], refs[12:21], refs[21]
    copies = []
    for i, (src, dst) in enumerate(zip(sources, kept)):
        src = src.at[blk[0]] if i == 6 else src
        copies.append(pltpu.make_async_copy(src, dst, sems.at[i]))
    for copy in copies:
        copy.start()
    for copy in copies:
        copy.wait()
    q_ref, k_ref, v_ref, docs_ref, qg_ref, kg_ref, row_ref, col_ref, norm_ref = kept
    gain_ref[...] = norm_ref[...]
    lane = iota((TOK, LANES), 1)
    low = lane < HD
    even = (lane & 1) == 0
    rows = row_ref[...]
    per = TOK // GRID_W
    cos_t = jnp.concatenate([col_ref[0] + rows[j : j + 1] for j in range(per)], axis=0)
    sin_t = jnp.concatenate([col_ref[1] + rows[per + j : per + j + 1] for j in range(per)], axis=0)

    def turn(n):
        swapped = jnp.where(even, pltpu.roll(n, LANES - 1, 1), pltpu.roll(n, 1, 1))
        return n * cos_t + swapped * sin_t

    x = q_ref[...].astype(F32)
    sq = x * x
    s0 = jnp.sum(jnp.where(low, sq, 0.0), axis=1, keepdims=True)
    s1 = jnp.sum(jnp.where(low, 0.0, sq), axis=1, keepdims=True)
    r0 = lax.rsqrt(s0 * (1.0 / HD) + EPSILON)
    r1 = lax.rsqrt(s1 * (1.0 / HD) + EPSILON)
    gain = jnp.concatenate([qg_ref[...], qg_ref[...]], axis=1)
    q_out = turn(x * jnp.where(low, r0, r1) * gain).astype(BF16)

    flat = k_ref[...].astype(F32)
    k = jnp.concatenate([flat, jnp.zeros_like(flat)], axis=0).T
    rk = lax.rsqrt(jnp.sum(k * k, axis=1, keepdims=True) * (1.0 / HD) + EPSILON)
    gain_k = jnp.concatenate([kg_ref[...], kg_ref[...]], axis=1)
    k = turn(k * rk * gain_k)
    keys = jnp.where(low[:HALF], k[:HALF], pltpu.roll(k[HALF:], HD, 1)).astype(BF16)
    values = v_ref[...]

    docs = docs_ref[...]
    n0 = jnp.sum((docs < 1).astype(F32))
    n1 = jnp.sum((docs < 2).astype(F32))
    row = iota((NOTE, LANES), 0)
    note = jnp.where(row == 0, n0, jnp.where(row == 1, n1, 0.0)).astype(BF16)
    qs_ref[:TOK, :] = q_out
    qs_ref[TOK:, :] = note
    for i in range(N_Z):
        kvs_ref[i, :HALF, :] = keys
        kvs_ref[i, HALF : HALF + HD, :] = values[:, :HALF]
        kvs_ref[i, HALF + HD : TOK, :] = values[:, HALF:]
        kvs_ref[i, TOK:, :] = note


def split3(x):
    hi = x.astype(BF16).astype(F32)
    mid = (x - hi).astype(BF16).astype(F32)
    return hi, mid, x - hi - mid


def attend_body(spot, *refs):
    q_refs, (kv_ref, out_ref, q_ref, kp_ref, vt_ref, score_ref, plan_ref) = refs[:N_X], refs[N_X:]
    for i in range(N_X):
        q_ref[i] = q_refs[i][...]
    lane = iota((TOK, LANES), 1)
    low = lane < HD
    idx = iota((TOK, LANES), 0).astype(F32)

    def doc_of(note):
        n0 = note[0:1, :].astype(F32)
        n1 = note[1:2, :].astype(F32)
        return jnp.where(idx < n0, HD, jnp.where(idx < n1, HD + 1, HD + 2))

    for j in range(N_Z):
        mark = (doc_of(kv_ref[j, TOK:, :]) == lane).astype(F32)
        pair = kv_ref[j, :HALF, :].astype(F32)
        kf = jnp.concatenate([pair, pltpu.roll(pair, HD, 1)], axis=0)
        kp_ref[j * TOK : (j + 1) * TOK, :] = jnp.where(low, kf, mark).astype(BF16)
        vt_ref[j, :HD, :HALF] = kv_ref[j, HALF : HALF + HD, :]
        vt_ref[j, :HD, HALF:] = kv_ref[j, HALF + HD : TOK, :]
        vt_ref[j, HD:, :] = jnp.ones((SUMS, TOK), BF16)

    def documents(note):
        n0, n1 = note[0:1, :].astype(F32), note[1:2, :].astype(F32)
        one = jnp.ones((1, LANES), F32)
        least = jnp.where(n0 <= 0.0, one, 0.0) + jnp.where(n1 <= 0.0, one, 0.0)
        most = jnp.where(n0 < TOK, one, 0.0) + jnp.where(n1 < TOK, one, 0.0)
        return least, most

    ranges = [documents(kv_ref[j, TOK:, :]) for j in range(N_Z)]
    for b in range(N_X):
        least, most = documents(q_ref[b, TOK:, :])
        first = jnp.full((1, LANES), float(N_Z), F32)
        last = jnp.full((1, LANES), -1.0, F32)
        for j, (low_doc, high_doc) in enumerate(ranges):
            meet = (low_doc <= most) & (least <= high_doc)
            first = jnp.where(meet, jnp.minimum(first, float(j)), first)
            last = jnp.where(meet, float(j), last)
        code = jnp.where(last < 0.0, 0.0, first * 16.0 + (last - first + 1.0))
        plan_ref[b] = jnp.max(code).astype(jnp.int32)
    note_row = iota((NOTE, HALF), 0)

    def block(b, start, size):
        qf = q_ref[b, :TOK, :].astype(F32) * (HD**-0.5)
        doc = doc_of(q_ref[b, TOK:, :])
        other = jnp.where((doc == lane) | (lane > HD + 2), 0.0, -MASK_BIG)
        heads = [jnp.where(low, qh, other).astype(BF16) for qh in (qf, pltpu.roll(qf, HD, 1))]
        peaks = [jnp.full((8, TOK), -jnp.inf, F32) for _ in heads]
        accs = [jnp.zeros((HD + SUMS, TOK), F32) for _ in heads]
        tops = [None, None]

        def score(h, j):
            at = pl.multiple_of((start + j) * TOK, TOK)
            part = dot(kp_ref[pl.ds(at, TOK), :], heads[h], 1, 1)
            score_ref[h, j] = part
            peaks[h] = jnp.maximum(peaks[h], jnp.max(part.reshape(TOK // 8, 8, TOK), axis=0))

        def weigh(h, j):
            p = jnp.exp(score_ref[h, j] - tops[h]).astype(BF16)
            accs[h] = accs[h] + dot(vt_ref[start + j], p)

        for j in range(size):
            score(0, j)
        tops[0] = jnp.max(peaks[0], axis=0, keepdims=True)
        for j in range(size):
            score(1, j)
            weigh(0, j)
        tops[1] = jnp.max(peaks[1], axis=0, keepdims=True)
        for j in range(size):
            weigh(1, j)
        peak = jnp.concatenate(tops, axis=1)
        total = jnp.concatenate([acc[HD : HD + 1, :] for acc in accs], axis=1)
        o = [acc[:HD, :] / acc[HD : HD + 1, :] for acc in accs]
        o = jnp.concatenate(o, axis=0).T.astype(BF16)
        terms = split3(peak + jnp.log(total))
        for half in range(2):
            stat = jnp.zeros((NOTE, HALF), F32)
            for i in range(6):
                at = (i // 3) * TOK + half * HALF
                stat = jnp.where(note_row == i, terms[i % 3][:, at : at + HALF], stat)
            to = lax.rem(spot[0] + N_X - b, N_X) * 2 + half
            out_ref[to, :HALF, :] = o[half * HALF : (half + 1) * HALF]
            out_ref[to, HALF:, :] = stat.astype(BF16)

    def step(b, carry):
        code = plan_ref[b]
        first, count = code // 16, code % 16
        fewer = -1
        for size in WINDOWS:

            @pl.when((count > fewer) & (count <= size))
            def _(size=size):
                start = 0 if size == N_Z else jnp.minimum(first, N_Z - size)
                block(b, start, size)

            fewer = size
        return carry

    lax.fori_loop(0, N_X, step, 0)


def project_body(core, in_ref, w_own_ref, w_other_ref, gain_ref, out_ref):
    gain = split3(gain_ref[...])
    row = iota((NOTE, LANES), 0)
    lane = iota((NOTE, LANES), 1)
    pick = (((row < 3) & (lane < HD)) | ((row >= 3) & (row < 6) & (lane >= HD))).astype(BF16)

    def attended(c):
        lse = [dot(in_ref[x * 2 + c, HALF:, :], pick, 0, 0) for x in range(N_X)]
        top = functools.reduce(jnp.maximum, lse)
        total = jnp.zeros((HALF, LANES), F32)
        mixed = jnp.zeros((HALF, LANES), F32)
        for x in range(N_X):
            w = jnp.exp(lse[x] - top)
            total = total + w
            mixed = mixed + w * in_ref[x * 2 + c, :HALF, :].astype(F32)
        return (mixed / total).astype(BF16)

    note = jnp.where(row == 0, gain[0], jnp.where(row == 1, gain[1], jnp.where(row == 2, gain[2], 0.0)))
    own = attended(core[0])
    other = attended(1 - core[0])
    for g in range(N_TP):
        cols = slice(g * LANES, (g + 1) * LANES)
        part = dot(own, w_own_ref[:, cols]) + dot(other, w_other_ref[:, cols])
        out_ref[g, :HALF, :] = part.astype(BF16)
        out_ref[g, HALF:, :] = note.astype(BF16)


def slots_of(routes_ref):
    expert = iota((EXPERTS, TOK), 0)
    r0, r1 = routes_ref[0:1, :], routes_ref[1:2, :]
    named = ((expert == r0) | (expert == r1)).astype(F32)
    before = (iota((TOK, TOK), 0) < iota((TOK, TOK), 1)).astype(BF16)
    slot = dot(named.astype(BF16), before)
    return expert == r0, expert == r1, jnp.where(named > 0.0, slot, -1.0)


def laid_out(slot, value, write):
    slots = iota((CAP_PAD, TOK), 0).astype(F32)
    for e in range(0, EXPERTS, 2):
        both = [jnp.where(slots == slot[i : i + 1, :], value(i), 0.0) for i in (e, e + 1)]
        write(slice(e * CAP_PAD, (e + 2) * CAP_PAD), jnp.concatenate(both, axis=0).astype(BF16))


def route_body(routes_ref, place_ref):
    _, _, slot = slots_of(routes_ref)

    def write(rows, value):
        place_ref[rows, :] = value

    laid_out(slot, lambda e: 1.0, write)


def mix_body(term, routes_ref, weight_ref, mix_ref):
    first, second, slot = slots_of(routes_ref)
    weight = jnp.where(first, weight_ref[0:1, :], jnp.where(second, weight_ref[1:2, :], 0.0))
    part = split3(weight)[term]

    parts = []
    laid_out(slot, lambda e: part[e : e + 1, :], lambda rows, value: parts.append(value))
    for i in range(0, len(parts), 8):
        some = jnp.concatenate(parts[i : i + 8], axis=0).astype(F32)
        mix_ref[:, i * 2 * CAP_PAD : (i + 8) * 2 * CAP_PAD] = some.T.astype(BF16)


def dispatch_body(in_ref, residual_ref, place_ref, mixed_ref, gain_ref, out_ref):
    halves = []
    for c in range(2):
        total = in_ref[c, :HALF, :].astype(F32)
        for y in range(1, N_Y):
            total = total + in_ref[y * 2 + c, :HALF, :].astype(F32)
        halves.append(total)
    for g in range(N_TP):
        note = in_ref[g, HALF:, :].astype(F32)
        gain = note[0:1] + note[1:2] + note[2:3]
        gain_ref[g] = jnp.broadcast_to(gain, (8, LANES))
    mixed = residual_ref[...].astype(F32) + jnp.concatenate(halves, axis=0)
    mixed_ref[...] = mixed
    out_ref[...] = dot(place_ref[...], mixed.astype(BF16)).astype(BF16)


def spread_body(in_ref, drop_ref, out_ref):
    span = BLOCKS * CAP_PAD
    for r in range(GROUPS):
        kept = dot(drop_ref[...], in_ref[r * span : (r + 1) * span, :]).astype(BF16)
        for g in range(r, N_TP, GROUPS):
            out_ref[g] = kept


def expert_body(in_ref, gain_ref, late0_ref, late1_ref, *refs):
    many = 3 * GROUPS - 2
    far, (out_ref, x_ref), weights, sems = refs[:many], refs[many : many + 2], refs[many + 2 : -1], refs[-1]
    copies = [pltpu.make_async_copy(far[i], weights[i], sems.at[i]) for i in range(many)]
    for copy in copies[:4]:
        copy.start()
    total = jnp.zeros((ROWS, LANES), F32)
    for g in range(N_TP):
        x = in_ref[g].astype(F32)
        total = total + x * x
    scale = lax.rsqrt(jnp.sum(total, axis=1, keepdims=True) * (1.0 / D) + EPSILON)
    for g in range(N_TP):
        x = in_ref[g].astype(F32) * scale * gain_ref[g, 0:1, :]
        x_ref[:, g * LANES : (g + 1) * LANES] = x.astype(BF16)
    hidden = []
    for i in range(GROUPS):
        copies[2 * i].wait()
        copies[2 * i + 1].wait()
        for copy in copies[2 * i + 4 : 2 * i + 6]:
            copy.start()
        gate = jnp.minimum(dot(x_ref[...], weights[2 * i][...]), CLAMP_LIMIT)
        up = jnp.clip(dot(x_ref[...], weights[2 * i + 1][...]), -CLAMP_LIMIT, CLAMP_LIMIT)
        unit = gate * (1.0 / (1.0 + jnp.exp(-SIGMOID_SCALE * gate))) * (up + 1.0)
        hidden.append(unit.astype(BF16))
    for copy in copies[2 * GROUPS :]:
        copy.wait()
    own_down, far_down = weights[2 * GROUPS :]
    downs = (own_down, late0_ref, far_down, late1_ref)
    for g in range(0, N_TP, 2):
        cols = slice(g * LANES, (g + 2) * LANES)
        part = dot(hidden[0], downs[0][:, cols])
        for h, w in zip(hidden[1:], downs[1:]):
            part = part + dot(h, w[:, cols])
        part = part.astype(BF16)
        out_ref[g] = part[:, :LANES]
        out_ref[g + 1] = part[:, LANES:]


def gather_body(in_ref, widen_ref, out_ref):
    span = BLOCKS * CAP_PAD
    for r in range(GROUPS):
        total = in_ref[r].astype(F32)
        for g in range(r + GROUPS, N_TP, GROUPS):
            total = total + in_ref[g].astype(F32)
        rows = dot(widen_ref[...], total.astype(BF16)).astype(BF16)
        out_ref[r * span : (r + 1) * span, :] = rows


def finish_body(in_ref, mix0_ref, mix1_ref, mix2_ref, mixed_ref, out_ref):
    total = mixed_ref[...]
    rows = in_ref[...]
    for mix_ref in (mix0_ref, mix1_ref, mix2_ref):
        total = total + dot(mix_ref[...], rows)
    out_ref[...] = total.astype(BF16)


def shaped(shape, dtype=BF16):
    return pltpu.VMEM(shape, dtype)


VMEM = pl.BlockSpec(memory_space=pltpu.VMEM)
SMEM = pl.BlockSpec(memory_space=pltpu.SMEM)
HBM = pl.BlockSpec(memory_space=pltpu.HBM)


def call(body, outs, *args, scratch=(), mib=8, far=0):
    near = len(args) - far
    specs = [SMEM if a.shape == (1,) else VMEM for a in args[:near]] + [HBM] * far
    args = args[:near] + tuple(pltpu.with_memory_space_constraint(a, pltpu.HBM) for a in args[near:])
    many = isinstance(outs, (list, tuple))
    return pl.pallas_call(
        body,
        out_shape=outs,
        in_specs=specs,
        out_specs=[VMEM] * len(outs) if many else VMEM,
        scratch_shapes=list(scratch),
        compiler_params=pltpu.CompilerParams(vmem_limit_bytes=mib * 1024 * 1024),
    )(*args)


def exchange(x, axes):
    return lax.all_to_all(x, axes, 0, 0, tiled=True)


def shifted(x, axis, size, by):
    return lax.ppermute(x, axis, [(i, (i + by) % size) for i in range(size)])


def partner(x):
    return lax.ppermute(x, "c", [(0, 1), (1, 0)])


def neighbour(x):
    pairs = []
    for y in range(N_Y):
        for c, to in ((0, y ^ 1), (1, (((y + 1) ^ 1) - 1) % N_Y)):
            pairs.append((y * N_C + c, to * N_C + c))
    return lax.ppermute(x, ("y", "c"), pairs)


def per_device(
    queries,
    keys,
    values,
    docs,
    query_gain,
    key_gain,
    out_weight,
    residual,
    norm_gain,
    routes,
    route_weight,
    gate_weight,
    up_weight,
    down_weight,
):
    return step(
        queries,
        keys.T,
        values.T,
        docs.reshape(2, LANES),
        query_gain.reshape(1, HD),
        key_gain.reshape(1, HD),
        out_weight,
        residual,
        norm_gain,
        routes.T,
        route_weight.T,
        gate_weight[0],
        up_weight[0],
        down_weight[0],
    )


def step(
    queries,
    keys,
    values,
    docs,
    query_gain,
    key_gain,
    out_weight,
    residual,
    norm_gain,
    routes,
    route_weight,
    gate,
    up,
    down,
):
    row_tab, col_tab = tables()
    drop = compaction()
    block = (lax.axis_index("z") * N_X + lax.axis_index("x")).reshape(1).astype(jnp.int32)
    spot = lax.axis_index("x").reshape(1).astype(jnp.int32)
    core = lax.axis_index("c").reshape(1).astype(jnp.int32)
    sources = (
        queries,
        keys,
        values,
        docs,
        query_gain,
        key_gain,
        jnp.asarray(row_tab),
        jnp.asarray(col_tab),
        norm_gain.reshape(1, LANES),
    )
    kept = [pltpu.VMEM(a.shape[1:] if i == 6 else a.shape, a.dtype) for i, a in enumerate(sources)]
    qs, kvs, gain_own = call(
        prep_body,
        [
            shaped((TOK + NOTE, LANES)),
            shaped((N_Z, TOK + NOTE, LANES)),
            shaped((1, LANES), F32),
        ],
        block,
        *sources,
        scratch=kept + [pltpu.SemaphoreType.DMA((len(sources),))],
        far=len(sources),
    )
    kv_all = exchange(kvs, "z")
    q_all = [qs] + [shifted(qs, "x", N_X, i) for i in range(1, N_X)]
    out_other = partner(out_weight)
    gate_y, up_y = neighbour(gate), neighbour(up)
    down_y = neighbour(down)
    gate_o, up_o = partner(gate), partner(up)
    down_o = partner(down)
    gate_yo, up_yo = partner(gate_y), partner(up_y)
    down_yo = partner(down_y)
    slot_table = shaped((EXPERTS * CAP_PAD, TOK))
    mix_table = shaped((TOK, EXPERTS * CAP_PAD))
    place = call(route_body, slot_table, routes)
    mixes = [
        call(functools.partial(mix_body, i), mix_table, routes, route_weight)
        for i in range(3)
    ]
    partial = call(
        attend_body,
        shaped((N_X * 2, HALF + NOTE, LANES)),
        spot,
        *q_all,
        kv_all,
        scratch=[
            pltpu.VMEM((N_X, TOK + NOTE, LANES), BF16),
            pltpu.VMEM((N_Z * TOK, LANES), BF16),
            pltpu.VMEM((N_Z, HD + SUMS, TOK), BF16),
            pltpu.VMEM((2, N_Z, TOK, TOK), F32),
            pltpu.SMEM((N_X,), jnp.int32),
        ],
        mib=24,
    )
    partial = exchange(partial, ("x", "c"))
    projected = call(
        project_body,
        shaped((N_TP, HALF + NOTE, LANES)),
        core,
        partial,
        out_weight,
        out_other,
        gain_own,
    )
    projected = exchange(projected, ("y", "c"))
    mixed, gain_all, outgoing = call(
        dispatch_body,
        [
            shaped((TOK, LANES), F32),
            shaped((N_TP, 8, LANES), F32),
            shaped((EXPERTS * CAP_PAD, LANES)),
        ],
        projected,
        residual,
        place,
    )
    arrived = exchange(outgoing.reshape(N_SP, CAP_PAD, LANES), ("z", "x"))
    spread = call(
        spread_body,
        shaped((N_TP, ROWS, LANES)),
        arrived.reshape(N_SP * CAP_PAD, LANES),
        jnp.asarray(drop, BF16),
    )
    columns = exchange(spread, ("y", "c"))
    weights = (gate, up, gate_o, up_o, gate_y, up_y, gate_yo, up_yo, down, down_y)
    parts = call(
        expert_body,
        shaped((N_TP, ROWS, LANES)),
        columns,
        gain_all,
        down_o,
        down_yo,
        *weights,
        scratch=[pltpu.VMEM((ROWS, D), BF16)]
        + [pltpu.VMEM(w.shape, BF16) for w in weights]
        + [pltpu.SemaphoreType.DMA((len(weights),))],
        mib=32,
        far=len(weights),
    )
    parts = exchange(parts, ("y", "c"))
    expert_out = call(
        gather_body, shaped((N_SP * CAP_PAD, LANES)), parts, jnp.asarray(drop.T, BF16)
    )
    returned = exchange(expert_out.reshape(N_SP, CAP_PAD, LANES), ("z", "x"))
    return call(
        finish_body,
        jax.ShapeDtypeStruct((TOK, LANES), BF16),
        returned.reshape(N_SP * CAP_PAD, LANES),
        *mixes,
        mixed,
    )


def solution(mesh):
    grid = Mesh(mesh.devices.reshape(N_Z, N_X, N_Y, N_C), ("z", "x", "y", "c"))
    sp, tp = ("z", "x"), ("y", "c")
    in_specs = (
        P(sp, tp),
        P(sp, tp),
        P(sp, tp),
        P(sp),
        P(),
        P(),
        P(tp, None),
        P(sp, tp),
        P(tp),
        P(sp, None),
        P(sp, None),
        P(sp, None, tp),
        P(sp, None, tp),
        P(sp, tp, None),
    )
    return jax.shard_map(
        per_device, mesh=grid, in_specs=in_specs, out_specs=P(sp, tp), check_vma=False
    )
```
